256 devices in a mesh: grp: 2 (over y), sp: 32 (over z, core), tp: 4 (over x).
Axes of the slice: x: 4, y: 2, z: 16, core: 2. Of those that a mesh axis runs over, the one named last changes fastest.
The devices are a block of a 4x16x16 slice.
Arguments:
- resid_in: bfloat16 [16384, 2048], P(('grp', 'sp', 'tp')), parts along dimension 0, may hold values from -3 to 3
- queries: bfloat16 [16384, 1024], P(('grp', 'sp'), 'tp'), parts along dimension 0, may hold values from -39 to 39
- keys: bfloat16 [16384, 1024], P(('grp', 'sp'), 'tp'), parts along dimension 0, may hold values from -6 to 6
- values: bfloat16 [16384, 1024], P(('grp', 'sp'), 'tp'), parts along dimension 0, may hold values from -12 to 12
- cum_gate: float32 [16384, 16], P('grp', 'tp'), parts along dimension 0, may hold values from -822 to 0, as said below
- w_out: bfloat16 [1024, 2048], replicated, may hold values from -0.1875 to 0.1875
- norm_gain: float32 [2048], replicated, may hold values from 0.1 to 1.9
- w_gate: bfloat16 [2048, 5632], P('sp', 'tp'), may hold values from -0.125 to 0.125
- w_up: bfloat16 [2048, 5632], P('sp', 'tp'), may hold values from -0.125 to 0.125
- w_down: bfloat16 [5632, 2048], P('tp', 'sp'), may hold values from -0.078125 to 0.078125
Outputs:
- resid_out: bfloat16 [16384, 2048], P(('grp', 'sp', 'tp')), parts along dimension 0
The draws below stay inside these ranges and needn't reach their ends.
There are 2 independent parts, one for each index of `grp`. The reference program is written for one: setup_inputs(seed, part) draws one part's arguments, and reference() takes and returns one part's arrays. A program takes and returns all parts, laid end to end along the dimension named above; an argument that names none is the same for every part. Nothing has to cross between parts.
Inputs may be any that keep to these rules, and one draw needn't show every extreme that they name: `cum_gate`: in every head the values never rise from one position to the next, and the first is at most 0.
All inputs are finite; a program needn't handle non-finite values.
Results may differ from the reference program's by a relative error of at most 0.018.
Values may be sent and summed in bfloat16 or wider, within the bound.
A program may use at most 128 MiB of HBM per device.

```python
import math
import jax
import jax.numpy as jnp
from jax import lax

D = 2048
HEADS = 16
HEAD_DIM = 64
FF = 5632
TOK_DEV = 256
SEQUENCE_TOKENS = 8192
ATT_WIDTH = 1024


def attention_pair(key):
    key_q, key_k = jax.random.split(key, 2)
    width = HEADS * HEAD_DIM
    queries = 2.0 * jnp.clip(jax.random.normal(key_q, (SEQUENCE_TOKENS, width), jnp.float32), -6.0, 6.0)
    keys = jnp.clip(jax.random.normal(key_k, (SEQUENCE_TOKENS, width), jnp.float32), -6.0, 6.0)
    return (queries, keys)


def draw_queries(key, part):
    return attention_pair(jax.random.fold_in(key, 11))[0].astype(jnp.bfloat16)


def draw_keys(key, part):
    return attention_pair(jax.random.fold_in(key, 11))[1].astype(jnp.bfloat16)


def draw_cum_gate(key, part):
    every_key_row = jax.random.split(jax.random.fold_in(key, 23), 6)
    sluggish_path = jax.random.permutation(every_key_row[0], HEADS) < HEADS // 2
    fast_rate = jnp.exp(jax.random.uniform(every_key_row[1], (HEADS,), jnp.float32, jnp.log(1.0 / 100.0), jnp.log(1.0 / 30.0)))
    rate = jnp.where(sluggish_path, 0.4 / SEQUENCE_TOKENS, fast_rate)
    factor = jnp.exp(jax.random.uniform(every_key_row[2], (SEQUENCE_TOKENS // TOK_DEV, 1), jnp.float32, jnp.log(0.5), jnp.log(2.0)))
    factor = jnp.repeat(factor, TOK_DEV, axis=0)
    rough = jax.random.uniform(every_key_row[3], (SEQUENCE_TOKENS, HEADS), jnp.float32, 0.5, 1.5)
    step_count = -rate[None, :] * factor * rough
    spike_position = jax.random.randint(every_key_row[4], (3,), 1, SEQUENCE_TOKENS, dtype=jnp.int32)
    training_loss = jax.random.uniform(every_key_row[5], (3, HEADS), jnp.float32, 0.2, 0.5)
    step_count = step_count.at[spike_position].add(jnp.log(1.0 - training_loss) * sluggish_path.astype(jnp.float32)[None, :])
    return jnp.cumsum(step_count, axis=0)


def levels(key, shape, cuts, low, top_value):
    factor_of, own = 1.0, jax.random.fold_in(key, 6)
    for position, shards_of in cuts:
        draws = jnp.exp(jax.random.uniform(jax.random.fold_in(own, position), (shards_of,), jnp.float32, low / len(cuts), top_value / len(cuts)))
        factor_of = factor_of * jnp.repeat(draws, shape[position] // shards_of).reshape([-1 if axis == position else 1 for axis in range(len(shape))])
    return factor_of


def scatter_about(key, shape, spread, reach, pieces=(), held_as=jnp.bfloat16):
    gain = levels(key, shape, pieces, -0.22, 0.18) if pieces else 1.0
    drawn = jax.random.normal(key, shape, jnp.float32) * spread * gain
    return jnp.minimum(jnp.maximum(drawn, -reach), reach).astype(held_as)


def setup_inputs(seed: int = 0, part: int = 0) -> dict:
    splits = jax.random.split(jax.random.key(seed), 11)
    part_splits = jax.random.split(jax.random.fold_in(splits[10], part), 11)
    return {
        "resid_in": scatter_about(part_splits[0], (SEQUENCE_TOKENS, D), 0.5, 3.0, ((0, 128),)),
        "queries": draw_queries(jax.random.fold_in(jax.random.fold_in(splits[10], part), 71), part),
        "keys": draw_keys(jax.random.fold_in(jax.random.fold_in(splits[10], part), 71), part),
        "values": scatter_about(part_splits[3], (SEQUENCE_TOKENS, ATT_WIDTH), 2.0, 12.0, ((0, 32), (1, 4))),
        "cum_gate": draw_cum_gate(jax.random.fold_in(jax.random.fold_in(splits[10], part), 71), part),
        "w_out": scatter_about(splits[5], (ATT_WIDTH, D), ATT_WIDTH ** -0.5, 0.1875),
        "norm_gain": jnp.clip(1.0 + 0.18 * jax.random.normal(splits[6], (D,), jnp.float32), 0.1, 1.9),
        "w_gate": scatter_about(splits[7], (D, FF), D ** -0.5, 0.125, ((0, 32), (1, 4))),
        "w_up": scatter_about(splits[8], (D, FF), D ** -0.5, 0.125, ((0, 32), (1, 4))),
        "w_down": scatter_about(splits[9], (FF, D), FF ** -0.5, 0.078125, ((0, 4), (1, 32))),
    }


def attention(queries, keys, values, cum_gate):
    total = queries.shape[0]
    span = math.gcd(total, 256)
    scale = HEAD_DIM ** (-0.5)
    query_heads = queries.astype(jnp.float32).reshape(total, HEADS, HEAD_DIM)
    key_heads = keys.astype(jnp.float32).reshape(total, HEADS, HEAD_DIM)
    value_heads = values.astype(jnp.float32).reshape(total, HEADS, HEAD_DIM)
    positions = jnp.arange(total, dtype=jnp.int32)

    def block(first):
        query_block = lax.dynamic_slice_in_dim(query_heads, first, span, 0)
        gate_block_rows = lax.dynamic_slice_in_dim(cum_gate, first, span, 0)
        scores = jnp.einsum('qhd,khd->hqk', query_block, key_heads) * scale
        scores = scores + gate_block_rows.T[:, :, None] - cum_gate.T[:, None, :]
        mask = positions[None, :] <= (first + jnp.arange(span, dtype=jnp.int32))[:, None]
        scores = jnp.where(mask[None], scores, -1e+30)
        top = lax.optimization_barrier(jnp.max(scores, axis=-1, keepdims=True))
        weights = jnp.where(mask[None], jnp.exp(scores - top), 0.0)
        totals = lax.optimization_barrier(jnp.sum(weights, axis=-1))
        rounded = lax.optimization_barrier(weights.astype(jnp.bfloat16)).astype(jnp.float32)
        attended = jnp.einsum('hqk,khd->qhd', rounded, value_heads) / totals.T[:, :, None]
        return attended.reshape(span, HEADS * HEAD_DIM).astype(jnp.bfloat16)
    starts = jnp.arange(total // span, dtype=jnp.int32) * span
    return lax.map(block, starts).reshape(total, HEADS * HEAD_DIM)

def reference(resid_in, queries, keys, values, cum_gate, w_out, norm_gain, w_gate, w_up, w_down):
    attended = attention(queries, keys, values, cum_gate)
    mixed = jnp.dot(attended, w_out, preferred_element_type=jnp.float32)
    resid = resid_in.astype(jnp.float32) + mixed
    normed = resid * lax.rsqrt(lax.optimization_barrier(jnp.mean(resid * resid, axis=-1, keepdims=True)) + 1e-06)
    normed = (normed * norm_gain).astype(jnp.bfloat16)
    gate = jnp.dot(normed, w_gate, preferred_element_type=jnp.float32)
    up = jnp.dot(normed, w_up, preferred_element_type=jnp.float32)
    hidden = (jax.nn.silu(gate) * up).astype(jnp.bfloat16)
    down = jnp.dot(hidden, w_down, preferred_element_type=jnp.float32)
    return (resid + down).astype(jnp.bfloat16)
```

```python
import functools

import jax
import jax.numpy as jnp
from jax import lax
from jax.experimental import pallas as pl
from jax.experimental.pallas import tpu as pltpu
from jax.sharding import PartitionSpec as P

HEAD_DIM = 64
NEG = -1e30
K, V, G, U, DA, DB = range(6)
UP, DOWN, OWN = range(3)
FAR = {K: UP, V: DOWN, G: UP, U: DOWN, DA: UP, DB: DOWN}
MESH = pl.DeviceIdType.MESH


def kernel(
    nz, ntp,
    resid_in, q_in, k_in, v_in, gate_in, wout_in, gain_in, wg_in, wu_in, wd_in,
    out_ref,
    kbuf, vbuf, wg, wu, wd, qbuf, qm, gate, wout, gain, resid0, resid,
    top, total, acc, att, head_rows, rows, acc_g, acc_u, hidden, terms, psend, precv,
    local_sem, ring_send, ring_recv, pair_send, pair_recv,
    att_send, att_recv, row_send, row_recv, sum_send, sum_recv,
):
    half = nz // 2
    me, t = lax.axis_index("sp"), lax.axis_index("tp")
    z, core = lax.div(me, 2), lax.rem(me, 2)
    partner = me + 1 - 2 * core
    neighbour = (
        2 * lax.rem(z + 1, nz) + core,
        2 * lax.rem(z + nz - 1, nz) + core,
    )
    tok, width = q_in.shape
    heads = width // HEAD_DIM
    own_rows, features = resid_in.shape
    depth, ff = wg_in.shape
    pair = 2 * depth

    def piece(kind, s):
        if kind == K:
            return kbuf.at[s]
        if kind == V:
            return vbuf.at[s]
        if kind == G:
            return wg.at[pl.ds(pl.multiple_of(s * depth, depth), depth)]
        if kind == U:
            return wu.at[pl.ds(pl.multiple_of(s * depth, depth), depth)]
        part = depth // 2
        return wd.at[pl.ds(pl.multiple_of(s * depth + (part if kind == DB else 0), part), part)]

    def owner(way, dist):
        if way == UP:
            return lax.rem(z + nz - dist, nz)
        return lax.rem(z + dist, nz)

    def ring_copy(kind, way, dist):
        ref = piece(kind, 2 * owner(way, dist - 1) + core)
        return pltpu.make_async_remote_copy(
            ref, ref, ring_send.at[kind, way, dist - 1], ring_recv.at[kind, way, dist - 1],
            device_id={"sp": neighbour[way]}, device_id_type=MESH,
        )

    def ring_wait(kind, way, dist):
        ref = piece(kind, 2 * owner(way, dist) + core)
        pltpu.make_async_remote_copy(
            ref, ref, ring_send.at[kind, way, dist - 1], ring_recv.at[kind, way, dist - 1],
            device_id={"sp": neighbour[way]}, device_id_type=MESH,
        ).wait_recv()

    def pair_copy(kind, way, dist, s):
        ref = piece(kind, s)
        return pltpu.make_async_remote_copy(
            ref, ref, pair_send.at[kind, way, dist - 1], pair_recv.at[kind, way, dist - 1],
            device_id={"sp": partner}, device_id_type=MESH,
        )

    def own_start(kind):
        for way in (UP, DOWN):
            ring_copy(kind, way, 1).start()
        pair_copy(kind, OWN, 1, me).start()

    def arrive(kind, dist):
        for way in (UP, DOWN):
            far = FAR[kind] == way

            def take(way=way, far=far):
                ring_wait(kind, way, dist)

                @pl.when(dist < (half if far else half - 1))
                def _():
                    ring_copy(kind, way, dist + 1).start()

                pair_copy(kind, way, dist, 2 * owner(way, dist) + core).start()

            if far:
                take()
            else:
                pl.when(dist < half)(take)

    def pair_wait(kind, way, dist):
        if way == OWN:
            s = partner
        else:
            s = 2 * owner(way, dist) + 1 - core
        pair_copy(kind, way, dist, s).wait_recv()

    def pair_waits(kinds, dist, ways=(UP, DOWN)):
        for kind in kinds:

            @pl.when(dist == 0)
            def _(kind=kind):
                pair_wait(kind, OWN, 1)

            @pl.when(dist == half)
            def _(kind=kind):
                pair_wait(kind, FAR[kind], half)

            @pl.when((dist > 0) & (dist < half))
            def _(kind=kind):
                for way in ways:
                    pair_wait(kind, way, dist)

    def mine(ref):
        return ref.at[pl.ds(pl.multiple_of(me * depth, depth), depth)]

    loads = [
        (k_in, kbuf.at[me]), (v_in, vbuf.at[me]), (q_in, qbuf), (gate_in, gate),
        (wg_in, mine(wg)), (wu_in, mine(wu)), (wd_in, mine(wd)),
        (resid_in, resid0), (wout_in, wout), (gain_in, gain),
    ]
    load = [pltpu.make_async_copy(a, b, local_sem.at[i]) for i, (a, b) in enumerate(loads)]
    for copy in load:
        copy.start()

    barrier = pltpu.get_barrier_semaphore()
    peers = [{"sp": neighbour[UP]}, {"sp": neighbour[DOWN]}, {"sp": partner}]
    across = [lax.rem(t + j, ntp) for j in range(1, ntp)]
    peers += [{"tp": other} for other in across]
    for peer in peers:
        pl.semaphore_signal(barrier, inc=1, device_id=peer, device_id_type=MESH)
    pl.semaphore_wait(barrier, len(peers))

    load[0].wait()
    own_start(K)
    load[1].wait()
    own_start(V)
    load[2].wait()
    load[3].wait()

    turned = (qbuf[...].astype(jnp.float32).T * HEAD_DIM ** (-0.5)).astype(jnp.bfloat16)
    nothing = jnp.zeros((HEAD_DIM, tok), jnp.bfloat16)
    for h in range(heads):
        mine_h = turned[h * HEAD_DIM : (h + 1) * HEAD_DIM]
        qm[h] = jnp.concatenate([mine_h, nothing] if h % 2 == 0 else [nothing, mine_h], axis=0)
    top[...] = jnp.full_like(top, NEG)
    total[...] = jnp.zeros_like(total)
    acc[...] = jnp.zeros_like(acc)

    def attend(s, diagonal):
        key_rows = kbuf[s]
        turned_values = vbuf[s].T
        bias = gate[:, pl.ds(pl.multiple_of(s * tok, tok), tok)]
        bias = jnp.concatenate([bias] * (8 // heads), axis=0).T
        for h in range(heads):
            lanes = slice(h // 2 * 128, h // 2 * 128 + 128)
            scores = jnp.dot(key_rows[:, lanes], qm[h], preferred_element_type=jnp.float32)
            scores = scores - bias[:, h : h + 1]
            if diagonal:
                at = lax.broadcasted_iota(jnp.int32, scores.shape, 0)
                scores = jnp.where(at <= lax.broadcasted_iota(jnp.int32, scores.shape, 1), scores, NEG)
            before = top[h : h + 1, :]
            now = jnp.maximum(before, jnp.max(scores, axis=0, keepdims=True))
            weights = jnp.exp(scores - now)
            rescale = jnp.exp(before - now)
            top[h : h + 1, :] = now
            total[h : h + 1, :] = total[h : h + 1, :] * rescale + jnp.sum(weights, axis=0, keepdims=True)
            part = slice(h * HEAD_DIM, (h + 1) * HEAD_DIM)
            product = jnp.dot(
                turned_values[part], weights.astype(jnp.bfloat16), preferred_element_type=jnp.float32
            )
            acc[part] = acc[part] * rescale + product

    attend(me, True)

    def attention_step(dist, carry):
        @pl.when(dist <= half)
        def _():
            arrive(K, dist)
            arrive(V, dist)

        @pl.when(dist == half - 1)
        def _():
            load[4].wait()
            own_start(G)
            load[5].wait()
            own_start(U)

        last = dist - 1
        pair_waits((K, V), last)

        def job(j, carry):
            way, par = lax.div(j, 2), lax.rem(j, 2)
            zb = lax.rem(z + nz + last * (2 * way - 1), nz)
            s = 2 * zb + core + par * (1 - 2 * core)

            @pl.when(s < me)
            def _():
                attend(s, False)

            return carry

        jobs = 4 - 2 * (lax.div(last, half) + lax.div(half - last, half))
        return lax.fori_loop(0, jobs, job, carry)

    lax.fori_loop(1, half + 2, attention_step, 0)

    sums = jnp.concatenate(
        [
            acc[h * HEAD_DIM : (h + 1) * HEAD_DIM] / total[h : h + 1, :]
            for h in range(heads)
        ],
        axis=0,
    )
    att[...] = sums.T.astype(jnp.bfloat16)

    def rows_of(ref, which):
        return ref.at[pl.ds(pl.multiple_of(which * own_rows, own_rows), own_rows)]

    def att_copy(j):
        return pltpu.make_async_remote_copy(
            rows_of(att, across[j]), head_rows.at[t], att_send.at[j], att_recv.at[j],
            device_id={"tp": across[j]}, device_id_type=MESH,
        )

    def att_wait(j):
        source = lax.rem(t + ntp - 1 - j, ntp)
        pltpu.make_async_remote_copy(
            rows_of(att, across[j]), head_rows.at[source], att_send.at[j], att_recv.at[j],
            device_id={"tp": across[j]}, device_id_type=MESH,
        ).wait_recv()

    arrive(G, 1)
    for j in range(ntp - 1):
        att_copy(j).start()
    head_rows[t] = att[pl.ds(pl.multiple_of(t * own_rows, own_rows), own_rows), :]
    load[7].wait()
    load[8].wait()
    load[9].wait()
    acc_g[...] = jnp.zeros_like(acc_g)
    acc_u[...] = jnp.zeros_like(acc_u)
    for j in range(ntp - 1):
        att_wait(j)
    tile = 256
    squares = jnp.zeros((own_rows, tile), jnp.float32)
    for i in range(features // tile):
        part = slice(i * tile, (i + 1) * tile)
        mixed = jnp.zeros((own_rows, tile), jnp.float32)
        for j in range(ntp):
            mixed += jnp.dot(
                head_rows[j], wout[j * width : (j + 1) * width, part],
                preferred_element_type=jnp.float32,
            )
        mixed = resid0[:, part].astype(jnp.float32) + mixed
        resid[:, part] = mixed
        squares += mixed * mixed
    scale = lax.rsqrt(jnp.sum(squares, axis=1, keepdims=True) / features + 1e-06)
    at_rows = pl.ds(pl.multiple_of(t * own_rows, own_rows), own_rows)
    rows[at_rows, :] = (resid[...] * scale * gain[...]).astype(jnp.bfloat16)

    def row_copy(j, which):
        return pltpu.make_async_remote_copy(
            rows_of(rows, which), rows_of(rows, which), row_send.at[j], row_recv.at[j],
            device_id={"tp": across[j]}, device_id_type=MESH,
        )

    arrive(U, 1)
    for j in range(ntp - 1):
        row_copy(j, t).start()

    def place(index):
        dist = lax.div(index + 1, 2)
        return dist, lax.rem(z + nz + dist * (1 - 2 * lax.rem(index, 2)), nz)

    def pair_ready(kinds, index, dist):
        for kind in kinds:

            @pl.when(dist == 0)
            def _(kind=kind):
                pair_wait(kind, OWN, 1)

            @pl.when(dist == half)
            def _(kind=kind):
                pair_wait(kind, FAR[kind], half)

            for way in (UP, DOWN):

                @pl.when((dist > 0) & (dist < half) & (lax.rem(index, 2) == 1 - way))
                def _(kind=kind, way=way):
                    pair_wait(kind, way, dist)

    first = 4

    def up_step(dist, carry):
        @pl.when(dist <= half)
        def _():
            arrive(G, dist)
            arrive(U, dist)

        @pl.when(dist == half - 1)
        def _():
            load[6].wait()
            own_start(DA)
            own_start(DB)

        @pl.when(dist == first)
        def _():
            for j in range(ntp - 1):
                row_copy(j, lax.rem(t + ntp - 1 - j, ntp)).wait_recv()

        def job(index, carry):
            away, zb = place(index)
            pair_ready((G, U), index, away)
            block = pl.ds(pl.multiple_of(zb * pair, pair), pair)
            left = rows[:, block]
            acc_g[...] += jnp.dot(left, wg[block, :], preferred_element_type=jnp.float32)
            acc_u[...] += jnp.dot(left, wu[block, :], preferred_element_type=jnp.float32)
            return carry

        started = jnp.where(dist < first, 0, 1)
        begin = jnp.where(dist <= first, 0, 2 * dist - 3)
        end = jnp.minimum(2 * dist - 1, nz) * started
        return lax.fori_loop(begin, end, job, carry)

    lax.fori_loop(2, half + 2, up_step, 0)

    def activate(i, carry):
        part = pl.ds(pl.multiple_of(i * 16, 16), 16)
        g = acc_g[part, :]
        hidden[part, :] = (g / (1.0 + jnp.exp(-g)) * acc_u[part, :]).astype(jnp.bfloat16)
        return carry

    lax.fori_loop(0, tok // 16, activate, 0)

    def sum_copy(j, zb):
        return pltpu.make_async_remote_copy(
            psend.at[zb, pl.ds(pl.multiple_of(across[j] * own_rows, own_rows), own_rows)],
            precv.at[j, zb], sum_send.at[j, zb], sum_recv.at[j, zb],
            device_id={"tp": across[j]}, device_id_type=MESH,
        )

    def down_step(dist, carry):
        @pl.when(dist <= half)
        def _():
            arrive(DA, dist)
            arrive(DB, dist)

        def job(index, carry):
            away, zb = place(index)
            pair_ready((DA, DB), index, away)
            block = pl.ds(pl.multiple_of(zb * pair, pair), pair)
            terms[...] = lax.dot_general(
                hidden[...], wd[block, :], (((1,), (1,)), ((), ())),
                preferred_element_type=jnp.float32,
            )
            psend[zb] = terms[...].astype(jnp.bfloat16)
            resid[:, block] += terms[at_rows, :]
            for j in range(ntp - 1):
                sum_copy(j, zb).start()
            return carry

        begin = jnp.maximum(2 * dist - 3, 0)
        lax.fori_loop(begin, jnp.minimum(2 * dist - 1, nz), job, carry)

        def finish(index, carry):
            _, zb = place(index)
            block = pl.ds(pl.multiple_of(zb * pair, pair), pair)
            value = resid[:, block]
            for j in range(ntp - 1):
                sum_copy(j, zb).wait_recv()
                value += precv[j, zb].astype(jnp.float32)
            out_ref[:, block] = value.astype(jnp.bfloat16)
            return carry

        begin = jnp.maximum(2 * dist - 5, 0)
        return lax.fori_loop(begin, jnp.clip(2 * dist - 3, 0, nz), finish, carry)

    lax.fori_loop(1, half + 3, down_step, 0)

    for j in range(ntp - 1):
        att_copy(j).wait_send()
        row_copy(j, t).wait_send()

    def sums_left(zb, carry):
        for j in range(ntp - 1):
            sum_copy(j, zb).wait_send()
        return carry

    lax.fori_loop(0, nz, sums_left, 0)
    for kind in range(6):
        pair_copy(kind, OWN, 1, me).wait_send()
        for way in (UP, DOWN):

            def left(dist, carry, kind=kind, way=way):
                ring_copy(kind, way, dist).wait_send()
                pair_copy(kind, way, dist, 2 * owner(way, dist) + core).wait_send()
                return carry

            lax.fori_loop(1, half + (1 if FAR[kind] == way else 0), left, 0)


def on_device(nsp, ntp, resid_in, queries, keys, values, cum_gate, w_out, norm_gain, w_gate, w_up, w_down):
    nz = nsp // 2
    half = nz // 2
    tok, width = queries.shape
    rows, features = resid_in.shape
    depth, ff = w_gate.shape
    heads = width // HEAD_DIM
    b16, f32 = jnp.bfloat16, jnp.float32
    dma = pltpu.SemaphoreType.DMA
    return pl.pallas_call(
        functools.partial(kernel, nz, ntp),
        out_shape=jax.ShapeDtypeStruct((rows, features), b16),
        in_specs=[pl.BlockSpec(memory_space=pl.ANY)] * 10,
        out_specs=pl.BlockSpec(memory_space=pltpu.VMEM),
        scratch_shapes=[
            pltpu.VMEM((nsp, tok, width), b16),
            pltpu.VMEM((nsp, tok, width), b16),
            pltpu.VMEM((nsp * depth, ff), b16),
            pltpu.VMEM((nsp * depth, ff), b16),
            pltpu.VMEM((nsp * depth, ff), b16),
            pltpu.VMEM((tok, width), b16),
            pltpu.VMEM((heads, 128, tok), b16),
            pltpu.VMEM((heads, nsp * tok), f32),
            pltpu.VMEM(w_out.shape, b16),
            pltpu.VMEM((1, features), f32),
            pltpu.VMEM((rows, features), b16),
            pltpu.VMEM((rows, features), f32),
            pltpu.VMEM((heads, tok), f32),
            pltpu.VMEM((heads, tok), f32),
            pltpu.VMEM((width, tok), f32),
            pltpu.VMEM((tok, width), b16),
            pltpu.VMEM((ntp, rows, width), b16),
            pltpu.VMEM((tok, features), b16),
            pltpu.VMEM((tok, ff), f32),
            pltpu.VMEM((tok, ff), f32),
            pltpu.VMEM((tok, ff), b16),
            pltpu.VMEM((tok, 2 * depth), f32),
            pltpu.VMEM((nz, tok, 2 * depth), b16),
            pltpu.VMEM((ntp - 1, nz, rows, 2 * depth), b16),
            dma((10,)),
            dma((6, 2, half)),
            dma((6, 2, half)),
            dma((6, 3, half)),
            dma((6, 3, half)),
            dma((ntp - 1,)),
            dma((ntp - 1,)),
            dma((ntp - 1,)),
            dma((ntp - 1,)),
            dma((ntp - 1, nz)),
            dma((ntp - 1, nz)),
        ],
        compiler_params=pltpu.CompilerParams(
            collective_id=0, has_side_effects=True, vmem_limit_bytes=60 * 1024 * 1024
        ),
        name="layer",
    )(
        resid_in, queries, keys, values, cum_gate.T, w_out, norm_gain[None, :], w_gate, w_up, w_down.T
    )


def solution(mesh):
    return jax.shard_map(
        functools.partial(on_device, mesh.shape["sp"], mesh.shape["tp"]),
        mesh=mesh,
        in_specs=(
            P(("grp", "sp", "tp"), None),
            P(("grp", "sp"), "tp"),
            P(("grp", "sp"), "tp"),
            P(("grp", "sp"), "tp"),
            P("grp", "tp"),
            P(),
            P(),
            P("sp", "tp"),
            P("sp", "tp"),
            P("tp", "sp"),
        ),
        out_specs=P(("grp", "sp", "tp"), None),
        check_vma=False,
    )
```

```python
import functools

import jax
import jax.numpy as jnp
from jax import lax
from jax.experimental import pallas as pl
from jax.experimental.pallas import tpu as pltpu
from jax.sharding import PartitionSpec as P

HEAD_DIM = 64
NEG = -1e30
K, V, G, U = range(4)
D = tuple(range(4, 8))
KINDS = 8
UP, DOWN, OWN = range(3)
FAR = {kind: kind % 2 for kind in range(KINDS)}
MESH = pl.DeviceIdType.MESH


def kernel(
    nz, ntp,
    resid_in, q_in, k_in, v_in, gate_in, wout_in, gain_in, wg_in, wu_in, wd_in,
    out_ref,
    kbuf, vbuf, wg, wu, wd, qbuf, qm, gate, wout, gain, resid0, resid,
    top, total, acc, att, head_rows, rows, acc_g, acc_u, hidden, terms, psend, precv,
    local_sem, ring_send, ring_recv, pair_send, pair_recv,
    att_send, att_recv, row_send, row_recv, sum_send, sum_recv,
):
    half = nz // 2
    mid = half // 2
    me, t = lax.axis_index("sp"), lax.axis_index("tp")
    z, core = lax.div(me, 2), lax.rem(me, 2)
    partner = me + 1 - 2 * core
    neighbour = (
        2 * lax.rem(z + 1, nz) + core,
        2 * lax.rem(z + nz - 1, nz) + core,
    )
    tok, width = q_in.shape
    heads = width // HEAD_DIM
    own_rows, features = resid_in.shape
    depth, ff = wg_in.shape
    pair = 2 * depth

    def piece(kind, s):
        if kind == K:
            return kbuf.at[s]
        if kind == V:
            return vbuf.at[s]
        if kind == G:
            return wg.at[pl.ds(pl.multiple_of(s * depth, depth), depth)]
        if kind == U:
            return wu.at[pl.ds(pl.multiple_of(s * depth, depth), depth)]
        part = depth // len(D)
        return wd.at[pl.ds(pl.multiple_of(s * depth + part * (kind - D[0]), part), part)]

    def owner(way, dist):
        if way == UP:
            return lax.rem(z + nz - dist, nz)
        return lax.rem(z + dist, nz)

    def ring_copy(kind, way, dist):
        ref = piece(kind, 2 * owner(way, dist - 1) + core)
        return pltpu.make_async_remote_copy(
            ref, ref, ring_send.at[kind, way, dist - 1], ring_recv.at[kind, way, dist - 1],
            device_id={"sp": neighbour[way]}, device_id_type=MESH,
        )

    def ring_wait(kind, way, dist):
        ref = piece(kind, 2 * owner(way, dist) + core)
        pltpu.make_async_remote_copy(
            ref, ref, ring_send.at[kind, way, dist - 1], ring_recv.at[kind, way, dist - 1],
            device_id={"sp": neighbour[way]}, device_id_type=MESH,
        ).wait_recv()

    def pair_copy(kind, way, dist, s):
        ref = piece(kind, s)
        return pltpu.make_async_remote_copy(
            ref, ref, pair_send.at[kind, way, dist - 1], pair_recv.at[kind, way, dist - 1],
            device_id={"sp": partner}, device_id_type=MESH,
        )

    def own_start(kind):
        for way in (UP, DOWN):
            ring_copy(kind, way, 1).start()
        pair_copy(kind, OWN, 1, me).start()

    def arrive(kind, dist):
        for way in (UP, DOWN):
            far = FAR[kind] == way

            def take(way=way, far=far):
                ring_wait(kind, way, dist)

                @pl.when(dist < (half if far else half - 1))
                def _():
                    ring_copy(kind, way, dist + 1).start()

                pair_copy(kind, way, dist, 2 * owner(way, dist) + core).start()

            if far:
                take()
            else:
                pl.when(dist < half)(take)

    def pair_wait(kind, way, dist):
        if way == OWN:
            s = partner
        else:
            s = 2 * owner(way, dist) + 1 - core
        pair_copy(kind, way, dist, s).wait_recv()

    def pair_waits(kinds, dist, ways=(UP, DOWN)):
        for kind in kinds:

            @pl.when(dist == 0)
            def _(kind=kind):
                pair_wait(kind, OWN, 1)

            @pl.when(dist == half)
            def _(kind=kind):
                pair_wait(kind, FAR[kind], half)

            @pl.when((dist > 0) & (dist < half))
            def _(kind=kind):
                for way in ways:
                    pair_wait(kind, way, dist)

    def mine(ref):
        return ref.at[pl.ds(pl.multiple_of(me * depth, depth), depth)]

    loads = [
        (k_in, kbuf.at[me]), (v_in, vbuf.at[me]), (q_in, qbuf), (gate_in, gate),
        (wg_in, mine(wg)), (wu_in, mine(wu)), (wd_in, mine(wd)),
        (resid_in, resid0), (wout_in, wout), (gain_in, gain),
    ]
    load = [pltpu.make_async_copy(a, b, local_sem.at[i]) for i, (a, b) in enumerate(loads)]
    for copy in load:
        copy.start()

    barrier = pltpu.get_barrier_semaphore()
    peers = [{"sp": neighbour[UP]}, {"sp": neighbour[DOWN]}, {"sp": partner}]
    across = [lax.rem(t + j, ntp) for j in range(1, ntp)]
    peers += [{"tp": other} for other in across]
    for peer in peers:
        pl.semaphore_signal(barrier, inc=1, device_id=peer, device_id_type=MESH)
    pl.semaphore_wait(barrier, len(peers))

    load[0].wait()
    own_start(K)
    load[1].wait()
    own_start(V)
    load[4].wait()
    own_start(G)
    load[2].wait()
    load[3].wait()

    turned = (qbuf[...].astype(jnp.float32).T * HEAD_DIM ** (-0.5)).astype(jnp.bfloat16)
    nothing = jnp.zeros((HEAD_DIM, tok), jnp.bfloat16)
    for h in range(heads):
        mine_h = turned[h * HEAD_DIM : (h + 1) * HEAD_DIM]
        qm[h] = jnp.concatenate([mine_h, nothing] if h % 2 == 0 else [nothing, mine_h], axis=0)
    top[...] = jnp.full_like(top, NEG)
    total[...] = jnp.zeros_like(total)
    acc[...] = jnp.zeros_like(acc)

    def attend(s, diagonal):
        key_rows = kbuf[s]
        turned_values = vbuf[s].T
        bias = gate[:, pl.ds(pl.multiple_of(s * tok, tok), tok)]
        bias = jnp.concatenate([bias] * (8 // heads), axis=0).T
        for h in range(heads):
            lanes = slice(h // 2 * 128, h // 2 * 128 + 128)
            scores = jnp.dot(key_rows[:, lanes], qm[h], preferred_element_type=jnp.float32)
            scores = scores - bias[:, h : h + 1]
            if diagonal:
                at = lax.broadcasted_iota(jnp.int32, scores.shape, 0)
                scores = jnp.where(at <= lax.broadcasted_iota(jnp.int32, scores.shape, 1), scores, NEG)
            before = top[h : h + 1, :]
            now = jnp.maximum(before, jnp.max(scores, axis=0, keepdims=True))
            weights = jnp.exp(scores - now)
            rescale = jnp.exp(before - now)
            top[h : h + 1, :] = now
            total[h : h + 1, :] = total[h : h + 1, :] * rescale + jnp.sum(weights, axis=0, keepdims=True)
            part = slice(h * HEAD_DIM, (h + 1) * HEAD_DIM)
            product = jnp.dot(
                turned_values[part], weights.astype(jnp.bfloat16), preferred_element_type=jnp.float32
            )
            acc[part] = acc[part] * rescale + product

    attend(me, True)

    def attention_step(dist, carry):
        @pl.when(dist <= half)
        def _():
            arrive(K, dist)
            arrive(V, dist)

        @pl.when(dist == 1)
        def _():
            load[5].wait()
            own_start(U)

        @pl.when((dist > 1) & (dist <= half))
        def _():
            pl.when(lax.rem(dist, 2) == 0)(lambda: arrive(G, lax.div(dist, 2)))
            pl.when(lax.rem(dist, 2) == 1)(lambda: arrive(U, lax.div(dist, 2)))

        @pl.when(dist == half)
        def _():
            load[6].wait()
            for kind in D:
                own_start(kind)

        last = dist - 1
        pair_waits((K, V), last)

        def job(j, carry):
            way, par = lax.div(j, 2), lax.rem(j, 2)
            zb = lax.rem(z + nz + last * (2 * way - 1), nz)
            s = 2 * zb + core + par * (1 - 2 * core)

            @pl.when(s < me)
            def _():
                attend(s, False)

            return carry

        jobs = 4 - 2 * (lax.div(last, half) + lax.div(half - last, half))
        return lax.fori_loop(0, jobs, job, carry)

    lax.fori_loop(1, half + 2, attention_step, 0)

    sums = jnp.concatenate(
        [
            acc[h * HEAD_DIM : (h + 1) * HEAD_DIM] / total[h : h + 1, :]
            for h in range(heads)
        ],
        axis=0,
    )
    att[...] = sums.T.astype(jnp.bfloat16)

    def rows_of(ref, which):
        return ref.at[pl.ds(pl.multiple_of(which * own_rows, own_rows), own_rows)]

    def att_copy(j):
        return pltpu.make_async_remote_copy(
            rows_of(att, across[j]), head_rows.at[t], att_send.at[j], att_recv.at[j],
            device_id={"tp": across[j]}, device_id_type=MESH,
        )

    def att_wait(j):
        source = lax.rem(t + ntp - 1 - j, ntp)
        pltpu.make_async_remote_copy(
            rows_of(att, across[j]), head_rows.at[source], att_send.at[j], att_recv.at[j],
            device_id={"tp": across[j]}, device_id_type=MESH,
        ).wait_recv()

    for j in range(ntp - 1):
        att_copy(j).start()
    arrive(U, mid)
    head_rows[t] = att[pl.ds(pl.multiple_of(t * own_rows, own_rows), own_rows), :]
    load[7].wait()
    load[8].wait()
    load[9].wait()
    acc_g[...] = jnp.zeros_like(acc_g)
    acc_u[...] = jnp.zeros_like(acc_u)
    for j in range(ntp - 1):
        att_wait(j)
    tile = 256
    squares = jnp.zeros((own_rows, tile), jnp.float32)
    for i in range(features // tile):
        part = slice(i * tile, (i + 1) * tile)
        mixed = jnp.zeros((own_rows, tile), jnp.float32)
        for j in range(ntp):
            mixed += jnp.dot(
                head_rows[j], wout[j * width : (j + 1) * width, part],
                preferred_element_type=jnp.float32,
            )
        mixed = resid0[:, part].astype(jnp.float32) + mixed
        resid[:, part] = mixed
        squares += mixed * mixed
    scale = lax.rsqrt(jnp.sum(squares, axis=1, keepdims=True) / features + 1e-06)
    at_rows = pl.ds(pl.multiple_of(t * own_rows, own_rows), own_rows)
    rows[at_rows, :] = (resid[...] * scale * gain[...]).astype(jnp.bfloat16)

    def row_copy(j, which):
        return pltpu.make_async_remote_copy(
            rows_of(rows, which), rows_of(rows, which), row_send.at[j], row_recv.at[j],
            device_id={"tp": across[j]}, device_id_type=MESH,
        )

    def forward_down(dist):
        for kind in D:
            arrive(kind, dist)

    arrive(G, mid + 1)
    for j in range(ntp - 1):
        row_copy(j, t).start()
    forward_down(1)

    def place(index):
        dist = lax.div(index + 1, 2)
        return dist, lax.rem(z + nz + dist * (1 - 2 * lax.rem(index, 2)), nz)

    def pair_ready(kinds, index, dist):
        for kind in kinds:

            @pl.when(dist == 0)
            def _(kind=kind):
                pair_wait(kind, OWN, 1)

            @pl.when(dist == half)
            def _(kind=kind):
                pair_wait(kind, FAR[kind], half)

            for way in (UP, DOWN):

                @pl.when((dist > 0) & (dist < half) & (lax.rem(index, 2) == 1 - way))
                def _(kind=kind, way=way):
                    pair_wait(kind, way, dist)

    first = mid + 2

    def up_step(dist, carry):
        @pl.when(dist <= half)
        def _():
            arrive(U, dist)

        @pl.when(dist < half)
        def _():
            arrive(G, dist + 1)

        @pl.when(dist <= half)
        def _():
            forward_down(dist - mid + 1)

        @pl.when(dist == first)
        def _():
            for j in range(ntp - 1):
                row_copy(j, lax.rem(t + ntp - 1 - j, ntp)).wait_recv()

        def job(index, carry):
            away, zb = place(index)
            pair_ready((G, U), index, away)
            block = pl.ds(pl.multiple_of(zb * pair, pair), pair)
            left = rows[:, block]
            acc_g[...] += jnp.dot(left, wg[block, :], preferred_element_type=jnp.float32)
            acc_u[...] += jnp.dot(left, wu[block, :], preferred_element_type=jnp.float32)
            return carry

        started = jnp.where(dist < first, 0, 1)
        begin = jnp.where(dist <= first, 0, 2 * dist - 3)
        end = jnp.minimum(2 * dist - 1, nz) * started
        return lax.fori_loop(begin, end, job, carry)

    lax.fori_loop(mid + 1, half + 2, up_step, 0)

    def activate(i, carry):
        part = pl.ds(pl.multiple_of(i * 16, 16), 16)
        g = acc_g[part, :]
        hidden[part, :] = (g / (1.0 + jnp.exp(-g)) * acc_u[part, :]).astype(jnp.bfloat16)
        return carry

    lax.fori_loop(0, tok // 16, activate, 0)

    def sum_copy(j, zb):
        return pltpu.make_async_remote_copy(
            psend.at[zb, pl.ds(pl.multiple_of(across[j] * own_rows, own_rows), own_rows)],
            precv.at[j, zb], sum_send.at[j, zb], sum_recv.at[j, zb],
            device_id={"tp": across[j]}, device_id_type=MESH,
        )

    start = half - mid + 2

    def down_step(dist, carry):
        @pl.when(dist <= half)
        def _():
            forward_down(dist)

        def job(index, carry):
            away, zb = place(index)
            pair_ready(D, index, away)
            block = pl.ds(pl.multiple_of(zb * pair, pair), pair)
            terms[...] = lax.dot_general(
                hidden[...], wd[block, :], (((1,), (1,)), ((), ())),
                preferred_element_type=jnp.float32,
            )
            psend[zb] = terms[...].astype(jnp.bfloat16)
            resid[:, block] += terms[at_rows, :]
            for j in range(ntp - 1):
                sum_copy(j, zb).start()
            return carry

        begin = jnp.where(dist == start, 0, 2 * dist - 3)
        lax.fori_loop(begin, jnp.minimum(2 * dist - 1, nz), job, carry)

        def finish(index, carry):
            _, zb = place(index)
            block = pl.ds(pl.multiple_of(zb * pair, pair), pair)
            value = resid[:, block]
            for j in range(ntp - 1):
                sum_copy(j, zb).wait_recv()
                value += precv[j, zb].astype(jnp.float32)
            out_ref[:, block] = value.astype(jnp.bfloat16)
            return carry

        begin = jnp.where(dist <= start + 1, 0, 2 * dist - 5)
        return lax.fori_loop(begin, jnp.where(dist == start, 0, jnp.minimum(2 * dist - 3, nz)), finish, carry)

    lax.fori_loop(start, half + 3, down_step, 0)

    for j in range(ntp - 1):
        att_copy(j).wait_send()
        row_copy(j, t).wait_send()

    def sums_left(zb, carry):
        for j in range(ntp - 1):
            sum_copy(j, zb).wait_send()
        return carry

    lax.fori_loop(0, nz, sums_left, 0)
    for kind in range(KINDS):
        pair_copy(kind, OWN, 1, me).wait_send()
        for way in (UP, DOWN):

            def left(dist, carry, kind=kind, way=way):
                ring_copy(kind, way, dist).wait_send()
                pair_copy(kind, way, dist, 2 * owner(way, dist) + core).wait_send()
                return carry

            lax.fori_loop(1, half + (1 if FAR[kind] == way else 0), left, 0)


def on_device(nsp, ntp, resid_in, queries, keys, values, cum_gate, w_out, norm_gain, w_gate, w_up, w_down):
    nz = nsp // 2
    half = nz // 2
    tok, width = queries.shape
    rows, features = resid_in.shape
    depth, ff = w_gate.shape
    heads = width // HEAD_DIM
    b16, f32 = jnp.bfloat16, jnp.float32
    dma = pltpu.SemaphoreType.DMA
    return pl.pallas_call(
        functools.partial(kernel, nz, ntp),
        out_shape=jax.ShapeDtypeStruct((rows, features), b16),
        in_specs=[pl.BlockSpec(memory_space=pl.ANY)] * 10,
        out_specs=pl.BlockSpec(memory_space=pltpu.VMEM),
        scratch_shapes=[
            pltpu.VMEM((nsp, tok, width), b16),
            pltpu.VMEM((nsp, tok, width), b16),
            pltpu.VMEM((nsp * depth, ff), b16),
            pltpu.VMEM((nsp * depth, ff), b16),
            pltpu.VMEM((nsp * depth, ff), b16),
            pltpu.VMEM((tok, width), b16),
            pltpu.VMEM((heads, 128, tok), b16),
            pltpu.VMEM((heads, nsp * tok), f32),
            pltpu.VMEM(w_out.shape, b16),
            pltpu.VMEM((1, features), f32),
            pltpu.VMEM((rows, features), b16),
            pltpu.VMEM((rows, features), f32),
            pltpu.VMEM((heads, tok), f32),
            pltpu.VMEM((heads, tok), f32),
            pltpu.VMEM((width, tok), f32),
            pltpu.VMEM((tok, width), b16),
            pltpu.VMEM((ntp, rows, width), b16),
            pltpu.VMEM((tok, features), b16),
            pltpu.VMEM((tok, ff), f32),
            pltpu.VMEM((tok, ff), f32),
            pltpu.VMEM((tok, ff), b16),
            pltpu.VMEM((tok, 2 * depth), f32),
            pltpu.VMEM((nz, tok, 2 * depth), b16),
            pltpu.VMEM((ntp - 1, nz, rows, 2 * depth), b16),
            dma((10,)),
            dma((KINDS, 2, half)),
            dma((KINDS, 2, half)),
            dma((KINDS, 3, half)),
            dma((KINDS, 3, half)),
            dma((ntp - 1,)),
            dma((ntp - 1,)),
            dma((ntp - 1,)),
            dma((ntp - 1,)),
            dma((ntp - 1, nz)),
            dma((ntp - 1, nz)),
        ],
        compiler_params=pltpu.CompilerParams(
            collective_id=0, has_side_effects=True, vmem_limit_bytes=60 * 1024 * 1024
        ),
        name="layer",
    )(
        resid_in, queries, keys, values, cum_gate.T, w_out, norm_gain[None, :], w_gate, w_up, w_down.T
    )


def solution(mesh):
    return jax.shard_map(
        functools.partial(on_device, mesh.shape["sp"], mesh.shape["tp"]),
        mesh=mesh,
        in_specs=(
            P(("grp", "sp", "tp"), None),
            P(("grp", "sp"), "tp"),
            P(("grp", "sp"), "tp"),
            P(("grp", "sp"), "tp"),
            P("grp", "tp"),
            P(),
            P(),
            P("sp", "tp"),
            P("sp", "tp"),
            P("tp", "sp"),
        ),
        out_specs=P(("grp", "sp", "tp"), None),
        check_vma=False,
    )
```

```python
import functools

import jax
import jax.numpy as jnp
from jax import lax
from jax.experimental import pallas as pl
from jax.experimental.pallas import tpu as pltpu
from jax.sharding import PartitionSpec as P

HEAD_DIM = 64
NEG = -1e30
K, V, G, U = range(4)
D = tuple(range(4, 8))
KINDS = 8
UP, DOWN, OWN = range(3)
FAR = {kind: kind % 2 for kind in range(KINDS)}
MESH = pl.DeviceIdType.MESH


def kernel(
    nz, ntp,
    resid_in, q_in, k_in, v_in, gate_in, wout_in, gain_in, wg_in, wu_in, wd_in,
    out_ref,
    kbuf, vbuf, wg, wu, wd, qbuf, qm, gate, wout, gain, resid0, resid,
    top, total, acc, att, head_rows, rows, acc_g, acc_u, hidden, terms, psend, precv,
    local_sem, ring_send, ring_recv, pair_send, pair_recv,
    att_send, att_recv, row_send, row_recv, sum_send, sum_recv,
):
    half = nz // 2
    mid = half // 2
    me, t = lax.axis_index("sp"), lax.axis_index("tp")
    z, core = lax.div(me, 2), lax.rem(me, 2)
    partner = me + 1 - 2 * core
    neighbour = (
        2 * lax.rem(z + 1, nz) + core,
        2 * lax.rem(z + nz - 1, nz) + core,
    )
    tok, width = q_in.shape
    heads = width // HEAD_DIM
    own_rows, features = resid_in.shape
    depth, ff = wg_in.shape
    pair = 2 * depth

    def piece(kind, s):
        if kind == K:
            return kbuf.at[s]
        if kind == V:
            return vbuf.at[s]
        if kind == G:
            return wg.at[pl.ds(pl.multiple_of(s * depth, depth), depth)]
        if kind == U:
            return wu.at[pl.ds(pl.multiple_of(s * depth, depth), depth)]
        part = depth // len(D)
        return wd.at[pl.ds(pl.multiple_of(s * depth + part * (kind - D[0]), part), part)]

    def owner(way, dist):
        if way == UP:
            return lax.rem(z + nz - dist, nz)
        return lax.rem(z + dist, nz)

    def ring_copy(kind, way, dist):
        ref = piece(kind, 2 * owner(way, dist - 1) + core)
        return pltpu.make_async_remote_copy(
            ref, ref, ring_send.at[kind, way, dist - 1], ring_recv.at[kind, way, dist - 1],
            device_id={"sp": neighbour[way]}, device_id_type=MESH,
        )

    def ring_wait(kind, way, dist):
        ref = piece(kind, 2 * owner(way, dist) + core)
        pltpu.make_async_remote_copy(
            ref, ref, ring_send.at[kind, way, dist - 1], ring_recv.at[kind, way, dist - 1],
            device_id={"sp": neighbour[way]}, device_id_type=MESH,
        ).wait_recv()

    def pair_copy(kind, way, dist, s):
        ref = piece(kind, s)
        return pltpu.make_async_remote_copy(
            ref, ref, pair_send.at[kind, way, dist - 1], pair_recv.at[kind, way, dist - 1],
            device_id={"sp": partner}, device_id_type=MESH,
        )

    def goes(kind, way, dist, s):
        if kind not in (K, V):
            return True
        if way == UP:
            return s + dist < nz
        return s < (half if FAR[kind] == way else half - 1)

    def used(kind, way, dist):
        return True if kind not in (K, V) else owner(way, dist) < z

    def guard(condition, run):
        if condition is True:
            run()
        else:
            pl.when(condition)(run)

    def own_start(kind):
        for way in (UP, DOWN):
            guard(goes(kind, way, 1, z), lambda way=way: ring_copy(kind, way, 1).start())
        pair_copy(kind, OWN, 1, me).start()

    def arrive(kind, dist):
        for way in (UP, DOWN):
            far = FAR[kind] == way
            s = owner(way, dist)

            def take(way=way, far=far, s=s):
                ring_wait(kind, way, dist)

                @pl.when(dist < (half if far else half - 1))
                def _():
                    guard(goes(kind, way, dist + 1, s), lambda: ring_copy(kind, way, dist + 1).start())

                guard(used(kind, way, dist), lambda: pair_copy(kind, way, dist, 2 * s + core).start())

            comes = goes(kind, way, dist, s)
            if far:
                guard(comes, take)
            else:
                pl.when(dist < half if comes is True else (dist < half) & comes)(take)

    def pair_wait(kind, way, dist):
        if way == OWN:
            pair_copy(kind, OWN, 1, partner).wait_recv()
        else:
            s = 2 * owner(way, dist) + 1 - core
            guard(used(kind, way, dist), lambda: pair_copy(kind, way, dist, s).wait_recv())

    def pair_waits(kinds, dist):
        for kind in kinds:

            @pl.when(dist == 0)
            def _(kind=kind):
                pair_wait(kind, OWN, 1)

            @pl.when(dist == half)
            def _(kind=kind):
                pair_wait(kind, FAR[kind], half)

            @pl.when((dist > 0) & (dist < half))
            def _(kind=kind):
                for way in (UP, DOWN):
                    pair_wait(kind, way, dist)

    def mine(ref):
        return ref.at[pl.ds(pl.multiple_of(me * depth, depth), depth)]

    loads = [
        (k_in, kbuf.at[me]), (v_in, vbuf.at[me]), (q_in, qbuf), (gate_in, gate),
        (wg_in, mine(wg)), (wu_in, mine(wu)), (wd_in, mine(wd)),
        (resid_in, resid0), (wout_in, wout), (gain_in, gain),
    ]
    load = [pltpu.make_async_copy(a, b, local_sem.at[i]) for i, (a, b) in enumerate(loads)]
    for copy in load:
        copy.start()

    barrier = pltpu.get_barrier_semaphore()
    peers = [{"sp": neighbour[UP]}, {"sp": neighbour[DOWN]}, {"sp": partner}]
    across = [lax.rem(t + j, ntp) for j in range(1, ntp)]
    peers += [{"tp": other} for other in across]
    for peer in peers:
        pl.semaphore_signal(barrier, inc=1, device_id=peer, device_id_type=MESH)
    pl.semaphore_wait(barrier, len(peers))

    load[0].wait()
    own_start(K)
    load[1].wait()
    own_start(V)
    load[4].wait()
    own_start(G)
    load[5].wait()
    own_start(U)
    load[2].wait()
    load[3].wait()

    turned = (qbuf[...].astype(jnp.float32).T * HEAD_DIM ** (-0.5)).astype(jnp.bfloat16)
    nothing = jnp.zeros((HEAD_DIM, tok), jnp.bfloat16)
    for h in range(heads):
        mine_h = turned[h * HEAD_DIM : (h + 1) * HEAD_DIM]
        qm[h] = jnp.concatenate([mine_h, nothing] if h % 2 == 0 else [nothing, mine_h], axis=0)
    top[...] = jnp.full_like(top, NEG)
    total[...] = jnp.zeros_like(total)
    acc[...] = jnp.zeros_like(acc)

    def attend(s, diagonal):
        key_rows = kbuf[s]
        turned_values = vbuf[s].T
        bias = gate[:, pl.ds(pl.multiple_of(s * tok, tok), tok)]
        bias = jnp.concatenate([bias] * (8 // heads), axis=0).T
        for h in range(heads):
            lanes = slice(h // 2 * 128, h // 2 * 128 + 128)
            scores = jnp.dot(key_rows[:, lanes], qm[h], preferred_element_type=jnp.float32)
            scores = scores - bias[:, h : h + 1]
            if diagonal:
                at = lax.broadcasted_iota(jnp.int32, scores.shape, 0)
                scores = jnp.where(at <= lax.broadcasted_iota(jnp.int32, scores.shape, 1), scores, NEG)
            before = top[h : h + 1, :]
            now = jnp.maximum(before, jnp.max(scores, axis=0, keepdims=True))
            weights = jnp.exp(scores - now)
            rescale = jnp.exp(before - now)
            top[h : h + 1, :] = now
            total[h : h + 1, :] = total[h : h + 1, :] * rescale + jnp.sum(weights, axis=0, keepdims=True)
            part = slice(h * HEAD_DIM, (h + 1) * HEAD_DIM)
            product = jnp.dot(
                turned_values[part], weights.astype(jnp.bfloat16), preferred_element_type=jnp.float32
            )
            acc[part] = acc[part] * rescale + product

    attend(me, True)

    def attention_step(dist, carry):
        @pl.when(dist <= half)
        def _():
            arrive(K, dist)
            arrive(V, dist)

        @pl.when((dist > 1) & (dist <= half))
        def _():
            pl.when(lax.rem(dist, 2) == 0)(lambda: arrive(G, lax.div(dist, 2)))
            pl.when(lax.rem(dist, 2) == 1)(lambda: arrive(U, lax.div(dist, 2)))

        @pl.when(dist == half)
        def _():
            load[6].wait()
            for kind in D:
                own_start(kind)

        last = dist - 1
        pair_waits((K, V), last)

        def job(j, carry):
            way, par = lax.div(j, 2), lax.rem(j, 2)
            zb = lax.rem(z + nz + last * (2 * way - 1), nz)
            s = 2 * zb + core + par * (1 - 2 * core)

            @pl.when(s < me)
            def _():
                attend(s, False)

            return carry

        jobs = 4 - 2 * (lax.div(last, half) + lax.div(half - last, half))
        return lax.fori_loop(0, jobs, job, carry)

    lax.fori_loop(1, half + 2, attention_step, 0)

    sums = jnp.concatenate(
        [
            acc[h * HEAD_DIM : (h + 1) * HEAD_DIM] / total[h : h + 1, :]
            for h in range(heads)
        ],
        axis=0,
    )
    att[...] = sums.T.astype(jnp.bfloat16)

    def rows_of(ref, which):
        return ref.at[pl.ds(pl.multiple_of(which * own_rows, own_rows), own_rows)]

    def att_copy(j):
        return pltpu.make_async_remote_copy(
            rows_of(att, across[j]), head_rows.at[t], att_send.at[j], att_recv.at[j],
            device_id={"tp": across[j]}, device_id_type=MESH,
        )

    def att_wait(j):
        source = lax.rem(t + ntp - 1 - j, ntp)
        pltpu.make_async_remote_copy(
            rows_of(att, across[j]), head_rows.at[source], att_send.at[j], att_recv.at[j],
            device_id={"tp": across[j]}, device_id_type=MESH,
        ).wait_recv()

    for j in range(ntp - 1):
        att_copy(j).start()
    arrive(U, mid)
    head_rows[t] = att[pl.ds(pl.multiple_of(t * own_rows, own_rows), own_rows), :]
    load[7].wait()
    load[8].wait()
    load[9].wait()
    acc_g[...] = jnp.zeros_like(acc_g)
    acc_u[...] = jnp.zeros_like(acc_u)
    for j in range(ntp - 1):
        att_wait(j)
    tile = 256
    squares = jnp.zeros((own_rows, tile), jnp.float32)
    for i in range(features // tile):
        part = slice(i * tile, (i + 1) * tile)
        mixed = jnp.zeros((own_rows, tile), jnp.float32)
        for j in range(ntp):
            mixed += jnp.dot(
                head_rows[j], wout[j * width : (j + 1) * width, part],
                preferred_element_type=jnp.float32,
            )
        mixed = resid0[:, part].astype(jnp.float32) + mixed
        resid[:, part] = mixed
        squares += mixed * mixed
    scale = lax.rsqrt(jnp.sum(squares, axis=1, keepdims=True) / features + 1e-06)
    at_rows = pl.ds(pl.multiple_of(t * own_rows, own_rows), own_rows)
    rows[at_rows, :] = (resid[...] * scale * gain[...]).astype(jnp.bfloat16)

    def row_copy(j, which):
        return pltpu.make_async_remote_copy(
            rows_of(rows, which), rows_of(rows, which), row_send.at[j], row_recv.at[j],
            device_id={"tp": across[j]}, device_id_type=MESH,
        )

    def forward_down(dist):
        for kind in D:
            arrive(kind, dist)

    arrive(G, mid + 1)
    for j in range(ntp - 1):
        row_copy(j, t).start()

    def place(index):
        dist = lax.div(index + 1, 2)
        return dist, lax.rem(z + nz + dist * (1 - 2 * lax.rem(index, 2)), nz)

    def pair_ready(kinds, index, dist):
        for kind in kinds:

            @pl.when(dist == 0)
            def _(kind=kind):
                pair_wait(kind, OWN, 1)

            @pl.when(dist == half)
            def _(kind=kind):
                pair_wait(kind, FAR[kind], half)

            for way in (UP, DOWN):

                @pl.when((dist > 0) & (dist < half) & (lax.rem(index, 2) == 1 - way))
                def _(kind=kind, way=way):
                    pair_wait(kind, way, dist)

    first = mid + 2

    def up_step(dist, carry):
        @pl.when(dist <= half)
        def _():
            arrive(U, dist)

        @pl.when(dist < half)
        def _():
            arrive(G, dist + 1)

        @pl.when((dist > mid + 1) & (dist <= half))
        def _():
            forward_down(dist - mid - 1)

        @pl.when(dist == first)
        def _():
            for j in range(ntp - 1):
                row_copy(j, lax.rem(t + ntp - 1 - j, ntp)).wait_recv()

        def job(index, carry):
            away, zb = place(index)
            pair_ready((G, U), index, away)
            block = pl.ds(pl.multiple_of(zb * pair, pair), pair)
            left = rows[:, block]
            acc_g[...] += jnp.dot(left, wg[block, :], preferred_element_type=jnp.float32)
            acc_u[...] += jnp.dot(left, wu[block, :], preferred_element_type=jnp.float32)
            return carry

        started = jnp.where(dist < first, 0, 1)
        begin = jnp.where(dist <= first, 0, 2 * dist - 3)
        end = jnp.minimum(2 * dist - 1, nz) * started
        return lax.fori_loop(begin, end, job, carry)

    lax.fori_loop(mid + 1, half + 2, up_step, 0)

    def activate(i, carry):
        part = pl.ds(pl.multiple_of(i * 16, 16), 16)
        g = acc_g[part, :]
        hidden[part, :] = (g / (1.0 + jnp.exp(-g)) * acc_u[part, :]).astype(jnp.bfloat16)
        return carry

    lax.fori_loop(0, tok // 16, activate, 0)

    def sum_copy(j, zb):
        return pltpu.make_async_remote_copy(
            psend.at[zb, pl.ds(pl.multiple_of(across[j] * own_rows, own_rows), own_rows)],
            precv.at[j, zb], sum_send.at[j, zb], sum_recv.at[j, zb],
            device_id={"tp": across[j]}, device_id_type=MESH,
        )

    start = half - mid

    def down_step(dist, carry):
        @pl.when(dist <= half)
        def _():
            forward_down(dist)

        def job(index, carry):
            away, zb = place(index)
            pair_ready(D, index, away)
            block = pl.ds(pl.multiple_of(zb * pair, pair), pair)
            terms[...] = lax.dot_general(
                hidden[...], wd[block, :], (((1,), (1,)), ((), ())),
                preferred_element_type=jnp.float32,
            )
            psend[zb] = terms[...].astype(jnp.bfloat16)
            resid[:, block] += terms[at_rows, :]
            for j in range(ntp - 1):
                sum_copy(j, zb).start()
            return carry

        begin = jnp.where(dist == start, 0, 2 * dist - 3)
        lax.fori_loop(begin, jnp.minimum(2 * dist - 1, nz), job, carry)

        def finish(index, carry):
            _, zb = place(index)
            block = pl.ds(pl.multiple_of(zb * pair, pair), pair)
            value = resid[:, block]
            for j in range(ntp - 1):
                sum_copy(j, zb).wait_recv()
                value += precv[j, zb].astype(jnp.float32)
            out_ref[:, block] = value.astype(jnp.bfloat16)
            return carry

        begin = jnp.where(dist <= start + 1, 0, 2 * dist - 5)
        return lax.fori_loop(begin, jnp.where(dist == start, 0, jnp.minimum(2 * dist - 3, nz)), finish, carry)

    lax.fori_loop(start, half + 3, down_step, 0)

    for j in range(ntp - 1):
        att_copy(j).wait_send()
        row_copy(j, t).wait_send()

    def sums_left(zb, carry):
        for j in range(ntp - 1):
            sum_copy(j, zb).wait_send()
        return carry

    lax.fori_loop(0, nz, sums_left, 0)
    for kind in range(KINDS):
        pair_copy(kind, OWN, 1, me).wait_send()
        for way in (UP, DOWN):

            def left(dist, carry, kind=kind, way=way):
                guard(
                    goes(kind, way, dist, owner(way, dist - 1)),
                    lambda: ring_copy(kind, way, dist).wait_send(),
                )
                guard(
                    used(kind, way, dist),
                    lambda: pair_copy(kind, way, dist, 2 * owner(way, dist) + core).wait_send(),
                )
                return carry

            lax.fori_loop(1, half + (1 if FAR[kind] == way else 0), left, 0)


def on_device(nsp, ntp, resid_in, queries, keys, values, cum_gate, w_out, norm_gain, w_gate, w_up, w_down):
    nz = nsp // 2
    half = nz // 2
    tok, width = queries.shape
    rows, features = resid_in.shape
    depth, ff = w_gate.shape
    heads = width // HEAD_DIM
    b16, f32 = jnp.bfloat16, jnp.float32
    dma = pltpu.SemaphoreType.DMA
    return pl.pallas_call(
        functools.partial(kernel, nz, ntp),
        out_shape=jax.ShapeDtypeStruct((rows, features), b16),
        in_specs=[pl.BlockSpec(memory_space=pl.ANY)] * 10,
        out_specs=pl.BlockSpec(memory_space=pltpu.VMEM),
        scratch_shapes=[
            pltpu.VMEM((nsp, tok, width), b16),
            pltpu.VMEM((nsp, tok, width), b16),
            pltpu.VMEM((nsp * depth, ff), b16),
            pltpu.VMEM((nsp * depth, ff), b16),
            pltpu.VMEM((nsp * depth, ff), b16),
            pltpu.VMEM((tok, width), b16),
            pltpu.VMEM((heads, 128, tok), b16),
            pltpu.VMEM((heads, nsp * tok), f32),
            pltpu.VMEM(w_out.shape, b16),
            pltpu.VMEM((1, features), f32),
            pltpu.VMEM((rows, features), b16),
            pltpu.VMEM((rows, features), f32),
            pltpu.VMEM((heads, tok), f32),
            pltpu.VMEM((heads, tok), f32),
            pltpu.VMEM((width, tok), f32),
            pltpu.VMEM((tok, width), b16),
            pltpu.VMEM((ntp, rows, width), b16),
            pltpu.VMEM((tok, features), b16),
            pltpu.VMEM((tok, ff), f32),
            pltpu.VMEM((tok, ff), f32),
            pltpu.VMEM((tok, ff), b16),
            pltpu.VMEM((tok, 2 * depth), f32),
            pltpu.VMEM((nz, tok, 2 * depth), b16),
            pltpu.VMEM((ntp - 1, nz, rows, 2 * depth), b16),
            dma((10,)),
            dma((KINDS, 2, half)),
            dma((KINDS, 2, half)),
            dma((KINDS, 3, half)),
            dma((KINDS, 3, half)),
            dma((ntp - 1,)),
            dma((ntp - 1,)),
            dma((ntp - 1,)),
            dma((ntp - 1,)),
            dma((ntp - 1, nz)),
            dma((ntp - 1, nz)),
        ],
        compiler_params=pltpu.CompilerParams(
            collective_id=0, has_side_effects=True, vmem_limit_bytes=60 * 1024 * 1024
        ),
        name="layer",
    )(
        resid_in, queries, keys, values, cum_gate.T, w_out, norm_gain[None, :], w_gate, w_up, w_down.T
    )


def solution(mesh):
    return jax.shard_map(
        functools.partial(on_device, mesh.shape["sp"], mesh.shape["tp"]),
        mesh=mesh,
        in_specs=(
            P(("grp", "sp", "tp"), None),
            P(("grp", "sp"), "tp"),
            P(("grp", "sp"), "tp"),
            P(("grp", "sp"), "tp"),
            P("grp", "tp"),
            P(),
            P(),
            P("sp", "tp"),
            P("sp", "tp"),
            P("tp", "sp"),
        ),
        out_specs=P(("grp", "sp", "tp"), None),
        check_vma=False,
    )
```

```python
import functools

import jax
import jax.numpy as jnp
from jax import lax
from jax.experimental import pallas as pl
from jax.experimental.pallas import tpu as pltpu
from jax.sharding import PartitionSpec as P

HEAD_DIM = 64
NEG = -1e30
K, V, G, U = range(4)
D = tuple(range(4, 8))
KINDS = 8
UP, DOWN, OWN = range(3)
FAR = {kind: kind % 2 for kind in range(KINDS)}
MESH = pl.DeviceIdType.MESH


def kernel(
    nz, ntp,
    resid_in, q_in, k_in, v_in, gate_in, wout_in, gain_in, wg_in, wu_in, wd_in,
    out_ref,
    kbuf, vbuf, wg, wu, wd, qbuf, qm, gate, wout, gain, resid0, resid,
    top, total, acc, att, head_rows, rows, acc_g, acc_u, hidden, terms, psend, precv,
    local_sem, ring_send, ring_recv, pair_send, pair_recv,
    att_send, att_recv, row_send, row_recv, sum_send, sum_recv,
):
    half = nz // 2
    mid = half // 2
    me, t = lax.axis_index("sp"), lax.axis_index("tp")
    z, core = lax.div(me, 2), lax.rem(me, 2)
    partner = me + 1 - 2 * core
    neighbour = (
        2 * lax.rem(z + 1, nz) + core,
        2 * lax.rem(z + nz - 1, nz) + core,
    )
    tok, width = q_in.shape
    heads = width // HEAD_DIM
    own_rows, features = resid_in.shape
    depth, ff = wg_in.shape
    pair = 2 * depth

    def piece(kind, s):
        if kind == K:
            return kbuf.at[s]
        if kind == V:
            return vbuf.at[s]
        if kind == G:
            return wg.at[pl.ds(pl.multiple_of(s * depth, depth), depth)]
        if kind == U:
            return wu.at[pl.ds(pl.multiple_of(s * depth, depth), depth)]
        part = depth // len(D)
        return wd.at[pl.ds(pl.multiple_of(s * depth + part * (kind - D[0]), part), part)]

    def owner(way, dist):
        if way == UP:
            return lax.rem(z + nz - dist, nz)
        return lax.rem(z + dist, nz)

    def ring_copy(kind, way, dist):
        ref = piece(kind, 2 * owner(way, dist - 1) + core)
        return pltpu.make_async_remote_copy(
            ref, ref, ring_send.at[kind, way, dist - 1], ring_recv.at[kind, way, dist - 1],
            device_id={"sp": neighbour[way]}, device_id_type=MESH,
        )

    def ring_wait(kind, way, dist):
        ref = piece(kind, 2 * owner(way, dist) + core)
        pltpu.make_async_remote_copy(
            ref, ref, ring_send.at[kind, way, dist - 1], ring_recv.at[kind, way, dist - 1],
            device_id={"sp": neighbour[way]}, device_id_type=MESH,
        ).wait_recv()

    def pair_copy(kind, way, dist, s):
        ref = piece(kind, s)
        return pltpu.make_async_remote_copy(
            ref, ref, pair_send.at[kind, way, dist - 1], pair_recv.at[kind, way, dist - 1],
            device_id={"sp": partner}, device_id_type=MESH,
        )

    def goes(kind, way, dist, s):
        if kind not in (K, V):
            return True
        if way == UP:
            return s + dist < nz
        return s < (half if FAR[kind] == way else half - 1)

    def used(kind, way, dist):
        return True if kind not in (K, V) else owner(way, dist) < z

    def guard(condition, run):
        if condition is True:
            run()
        else:
            pl.when(condition)(run)

    def own_start(kind):
        for way in (UP, DOWN):
            guard(goes(kind, way, 1, z), lambda way=way: ring_copy(kind, way, 1).start())
        pair_copy(kind, OWN, 1, me).start()

    def arrive(kind, dist):
        for way in (UP, DOWN):
            far = FAR[kind] == way
            s = owner(way, dist)

            def take(way=way, far=far, s=s):
                ring_wait(kind, way, dist)

                @pl.when(dist < (half if far else half - 1))
                def _():
                    guard(goes(kind, way, dist + 1, s), lambda: ring_copy(kind, way, dist + 1).start())

                guard(used(kind, way, dist), lambda: pair_copy(kind, way, dist, 2 * s + core).start())

            comes = goes(kind, way, dist, s)
            if far:
                guard(comes, take)
            else:
                pl.when(dist < half if comes is True else (dist < half) & comes)(take)

    def pair_wait(kind, way, dist):
        if way == OWN:
            pair_copy(kind, OWN, 1, partner).wait_recv()
        else:
            s = 2 * owner(way, dist) + 1 - core
            guard(used(kind, way, dist), lambda: pair_copy(kind, way, dist, s).wait_recv())

    def pair_waits(kinds, dist):
        for kind in kinds:

            @pl.when(dist == 0)
            def _(kind=kind):
                pair_wait(kind, OWN, 1)

            @pl.when(dist == half)
            def _(kind=kind):
                pair_wait(kind, FAR[kind], half)

            @pl.when((dist > 0) & (dist < half))
            def _(kind=kind):
                for way in (UP, DOWN):
                    pair_wait(kind, way, dist)

    def mine(ref):
        return ref.at[pl.ds(pl.multiple_of(me * depth, depth), depth)]

    loads = [
        (k_in, kbuf.at[me]), (v_in, vbuf.at[me]), (q_in, qbuf), (gate_in, gate),
        (wg_in, mine(wg)), (wu_in, mine(wu)), (wd_in, mine(wd)),
        (resid_in, resid0), (wout_in, wout), (gain_in, gain),
    ]
    load = [pltpu.make_async_copy(a, b, local_sem.at[i]) for i, (a, b) in enumerate(loads)]
    for copy in load:
        copy.start()

    barrier = pltpu.get_barrier_semaphore()
    peers = [{"sp": neighbour[UP]}, {"sp": neighbour[DOWN]}, {"sp": partner}]
    across = [lax.rem(t + j, ntp) for j in range(1, ntp)]
    peers += [{"tp": other} for other in across]
    for peer in peers:
        pl.semaphore_signal(barrier, inc=1, device_id=peer, device_id_type=MESH)
    pl.semaphore_wait(barrier, len(peers))

    load[0].wait()
    own_start(K)
    load[1].wait()
    own_start(V)
    load[4].wait()
    own_start(G)
    load[5].wait()
    own_start(U)
    load[2].wait()
    load[3].wait()

    turned = (qbuf[...].astype(jnp.float32).T * HEAD_DIM ** (-0.5)).astype(jnp.bfloat16)
    nothing = jnp.zeros((HEAD_DIM, tok), jnp.bfloat16)
    for h in range(heads):
        mine_h = turned[h * HEAD_DIM : (h + 1) * HEAD_DIM]
        qm[h] = jnp.concatenate([mine_h, nothing] if h % 2 == 0 else [nothing, mine_h], axis=0)
    top[...] = jnp.full_like(top, NEG)
    total[...] = jnp.zeros_like(total)
    acc[...] = jnp.zeros_like(acc)

    def attend(s, diagonal):
        key_rows = kbuf[s]
        turned_values = vbuf[s].T
        bias = gate[:, pl.ds(pl.multiple_of(s * tok, tok), tok)]
        bias = jnp.concatenate([bias] * (8 // heads), axis=0).T
        for h in range(heads):
            lanes = slice(h // 2 * 128, h // 2 * 128 + 128)
            scores = jnp.dot(key_rows[:, lanes], qm[h], preferred_element_type=jnp.float32)
            scores = scores - bias[:, h : h + 1]
            if diagonal:
                at = lax.broadcasted_iota(jnp.int32, scores.shape, 0)
                scores = jnp.where(at <= lax.broadcasted_iota(jnp.int32, scores.shape, 1), scores, NEG)
            before = top[h : h + 1, :]
            now = jnp.maximum(before, jnp.max(scores, axis=0, keepdims=True))
            weights = jnp.exp(scores - now)
            rescale = jnp.exp(before - now)
            top[h : h + 1, :] = now
            total[h : h + 1, :] = total[h : h + 1, :] * rescale + jnp.sum(weights, axis=0, keepdims=True)
            part = slice(h * HEAD_DIM, (h + 1) * HEAD_DIM)
            product = jnp.dot(
                turned_values[part], weights.astype(jnp.bfloat16), preferred_element_type=jnp.float32
            )
            acc[part] = acc[part] * rescale + product

    attend(me, True)

    def attention_step(dist, carry):
        @pl.when(dist <= half)
        def _():
            arrive(K, dist)
            arrive(V, dist)

        @pl.when((dist > 1) & (dist <= half))
        def _():
            pl.when(lax.rem(dist, 2) == 0)(lambda: arrive(G, lax.div(dist, 2)))
            pl.when(lax.rem(dist, 2) == 1)(lambda: arrive(U, lax.div(dist, 2)))

        @pl.when(dist == half)
        def _():
            load[6].wait()
            for kind in D:
                own_start(kind)

        last = dist - 1
        pair_waits((K, V), last)

        def job(j, carry):
            way, par = lax.div(j, 2), lax.rem(j, 2)
            zb = lax.rem(z + nz + last * (2 * way - 1), nz)
            s = 2 * zb + core + par * (1 - 2 * core)

            @pl.when(s < me)
            def _():
                attend(s, False)

            return carry

        jobs = 4 - 2 * (lax.div(last, half) + lax.div(half - last, half))
        return lax.fori_loop(0, jobs, job, carry)

    lax.fori_loop(1, half + 2, attention_step, 0)

    sums = jnp.concatenate(
        [
            acc[h * HEAD_DIM : (h + 1) * HEAD_DIM] / total[h : h + 1, :]
            for h in range(heads)
        ],
        axis=0,
    )
    att[...] = sums.T.astype(jnp.bfloat16)

    def rows_of(ref, which):
        return ref.at[pl.ds(pl.multiple_of(which * own_rows, own_rows), own_rows)]

    def att_copy(j):
        return pltpu.make_async_remote_copy(
            rows_of(att, across[j]), head_rows.at[t], att_send.at[j], att_recv.at[j],
            device_id={"tp": across[j]}, device_id_type=MESH,
        )

    def att_wait(j):
        source = lax.rem(t + ntp - 1 - j, ntp)
        pltpu.make_async_remote_copy(
            rows_of(att, across[j]), head_rows.at[source], att_send.at[j], att_recv.at[j],
            device_id={"tp": across[j]}, device_id_type=MESH,
        ).wait_recv()

    for j in range(ntp - 1):
        att_copy(j).start()
    arrive(U, mid)
    head_rows[t] = att[pl.ds(pl.multiple_of(t * own_rows, own_rows), own_rows), :]
    load[7].wait()
    load[8].wait()
    load[9].wait()
    acc_g[...] = jnp.zeros_like(acc_g)
    acc_u[...] = jnp.zeros_like(acc_u)
    for j in range(ntp - 1):
        att_wait(j)
    tile = 256
    squares = jnp.zeros((own_rows, tile), jnp.float32)
    for i in range(features // tile):
        part = slice(i * tile, (i + 1) * tile)
        mixed = jnp.zeros((own_rows, tile), jnp.float32)
        for j in range(ntp):
            mixed += jnp.dot(
                head_rows[j], wout[j * width : (j + 1) * width, part],
                preferred_element_type=jnp.float32,
            )
        mixed = resid0[:, part].astype(jnp.float32) + mixed
        resid[:, part] = mixed
        squares += mixed * mixed
    scale = lax.rsqrt(jnp.sum(squares, axis=1, keepdims=True) / features + 1e-06)
    at_rows = pl.ds(pl.multiple_of(t * own_rows, own_rows), own_rows)
    rows[at_rows, :] = (resid[...] * scale * gain[...]).astype(jnp.bfloat16)

    def row_copy(j, which):
        return pltpu.make_async_remote_copy(
            rows_of(rows, which), rows_of(rows, which), row_send.at[j], row_recv.at[j],
            device_id={"tp": across[j]}, device_id_type=MESH,
        )

    def forward_down(dist):
        for kind in D:
            arrive(kind, dist)

    arrive(G, mid + 1)
    for j in range(ntp - 1):
        row_copy(j, t).start()

    def place(index):
        dist = lax.div(index + 1, 2)
        return dist, lax.rem(z + nz + dist * (1 - 2 * lax.rem(index, 2)), nz)

    def pair_ready(kinds, index, dist):
        for kind in kinds:

            @pl.when(dist == 0)
            def _(kind=kind):
                pair_wait(kind, OWN, 1)

            @pl.when(dist == half)
            def _(kind=kind):
                pair_wait(kind, FAR[kind], half)

            for way in (UP, DOWN):

                @pl.when((dist > 0) & (dist < half) & (lax.rem(index, 2) == 1 - way))
                def _(kind=kind, way=way):
                    pair_wait(kind, way, dist)

    first, turns = mid + 2, 6

    def up_done(dist):
        return jnp.clip(jnp.minimum(turns * (dist - first + 1), 2 * dist - 1), 0, nz)

    def up_step(dist, carry):
        def turn(j, carry):
            @pl.when((j == 0) & (dist <= half))
            def _():
                arrive(U, dist)

            @pl.when((j == 2) & (dist < half))
            def _():
                arrive(G, dist + 1)

            @pl.when((j == 4) & (dist > mid + 1) & (dist <= half))
            def _():
                forward_down(dist - mid - 1)

            @pl.when((j == 4) & (dist == half - 1))
            def _():
                for i in range(ntp - 1):
                    att_copy(i).wait_send()

            @pl.when((j == 0) & (dist == first))
            def _():
                for i in range(ntp - 1):
                    row_copy(i, lax.rem(t + ntp - 1 - i, ntp)).wait_recv()

            index = up_done(dist - 1) + j

            @pl.when(index < up_done(dist))
            def _():
                away, zb = place(index)
                pair_ready((G, U), index, away)
                block = pl.ds(pl.multiple_of(zb * pair, pair), pair)
                left = rows[:, block]
                acc_g[...] += jnp.dot(left, wg[block, :], preferred_element_type=jnp.float32)
                acc_u[...] += jnp.dot(left, wu[block, :], preferred_element_type=jnp.float32)

            return carry

        return lax.fori_loop(0, turns, turn, carry)

    lax.fori_loop(mid + 1, half + 2, up_step, 0)

    def activate(i, carry):
        part = pl.ds(pl.multiple_of(i * 16, 16), 16)
        g = acc_g[part, :]
        hidden[part, :] = (g / (1.0 + jnp.exp(-g)) * acc_u[part, :]).astype(jnp.bfloat16)
        return carry

    lax.fori_loop(0, tok // 16, activate, 0)

    def sum_copy(j, zb):
        return pltpu.make_async_remote_copy(
            psend.at[zb, pl.ds(pl.multiple_of(across[j] * own_rows, own_rows), own_rows)],
            precv.at[j, zb], sum_send.at[j, zb], sum_recv.at[j, zb],
            device_id={"tp": across[j]}, device_id_type=MESH,
        )

    start = half - mid

    def down_done(dist):
        return jnp.clip(jnp.minimum(len(D) * (dist - start + 1), 2 * dist - 1), 0, nz)

    def sent(kinds, begin, end):
        for kind in kinds:
            for way in (UP, DOWN):

                def left(dist, carry, kind=kind, way=way):
                    guard(
                        goes(kind, way, dist, owner(way, dist - 1)),
                        lambda: ring_copy(kind, way, dist).wait_send(),
                    )
                    guard(
                        used(kind, way, dist),
                        lambda: pair_copy(kind, way, dist, 2 * owner(way, dist) + core).wait_send(),
                    )
                    return carry

                reach = half if FAR[kind] == way else half - 1
                lax.fori_loop(begin, min(end, reach + 1), left, 0)

    def down_step(dist, carry):
        def turn(j, carry):
            for i, kind in enumerate(D):

                @pl.when((j == i) & (dist <= half))
                def _(kind=kind):
                    arrive(kind, dist)

            index = down_done(dist - 1) + j

            @pl.when(index < down_done(dist))
            def _():
                away, zb = place(index)
                pair_ready(D, index, away)
                block = pl.ds(pl.multiple_of(zb * pair, pair), pair)
                terms[...] = lax.dot_general(
                    hidden[...], wd[block, :], (((1,), (1,)), ((), ())),
                    preferred_element_type=jnp.float32,
                )
                psend[zb] = terms[...].astype(jnp.bfloat16)
                resid[:, block] += terms[at_rows, :]
                for i in range(ntp - 1):
                    sum_copy(i, zb).start()

            return carry

        lax.fori_loop(0, len(D), turn, 0)

        @pl.when(dist == start)
        def _():
            for j in range(ntp - 1):
                row_copy(j, t).wait_send()
            for kind in range(KINDS):
                pair_copy(kind, OWN, 1, me).wait_send()
            sent((K, V), 1, half + 1)

        pl.when(dist == start + 1)(lambda: sent((G,), 1, half + 1))
        pl.when(dist == start + 2)(lambda: sent((U,), 1, half + 1))
        pl.when(dist == half - 1)(lambda: sent(D, 1, half - 1))
        pl.when(dist == half)(lambda: sent(D, half - 1, half))

        def finish(index, carry):
            _, zb = place(index)
            block = pl.ds(pl.multiple_of(zb * pair, pair), pair)
            value = resid[:, block]
            for j in range(ntp - 1):
                sum_copy(j, zb).wait_recv()
                sum_copy(j, zb).wait_send()
                value += precv[j, zb].astype(jnp.float32)
            out_ref[:, block] = value.astype(jnp.bfloat16)
            return carry

        return lax.fori_loop(down_done(dist - 2), down_done(dist - 1), finish, carry)

    lax.fori_loop(start, half + 3, down_step, 0)

    for kind in D:
        sent((kind,), half, half + 1)


def on_device(nsp, ntp, resid_in, queries, keys, values, cum_gate, w_out, norm_gain, w_gate, w_up, w_down):
    nz = nsp // 2
    half = nz // 2
    tok, width = queries.shape
    rows, features = resid_in.shape
    depth, ff = w_gate.shape
    heads = width // HEAD_DIM
    b16, f32 = jnp.bfloat16, jnp.float32
    dma = pltpu.SemaphoreType.DMA
    return pl.pallas_call(
        functools.partial(kernel, nz, ntp),
        out_shape=pltpu.VMEM((rows, features), b16),
        in_specs=[pl.BlockSpec(memory_space=pl.ANY)] * 10,
        out_specs=pl.BlockSpec(memory_space=pltpu.VMEM),
        scratch_shapes=[
            pltpu.VMEM((nsp, tok, width), b16),
            pltpu.VMEM((nsp, tok, width), b16),
            pltpu.VMEM((nsp * depth, ff), b16),
            pltpu.VMEM((nsp * depth, ff), b16),
            pltpu.VMEM((nsp * depth, ff), b16),
            pltpu.VMEM((tok, width), b16),
            pltpu.VMEM((heads, 128, tok), b16),
            pltpu.VMEM((heads, nsp * tok), f32),
            pltpu.VMEM(w_out.shape, b16),
            pltpu.VMEM((1, features), f32),
            pltpu.VMEM((rows, features), b16),
            pltpu.VMEM((rows, features), f32),
            pltpu.VMEM((heads, tok), f32),
            pltpu.VMEM((heads, tok), f32),
            pltpu.VMEM((width, tok), f32),
            pltpu.VMEM((tok, width), b16),
            pltpu.VMEM((ntp, rows, width), b16),
            pltpu.VMEM((tok, features), b16),
            pltpu.VMEM((tok, ff), f32),
            pltpu.VMEM((tok, ff), f32),
            pltpu.VMEM((tok, ff), b16),
            pltpu.VMEM((tok, 2 * depth), f32),
            pltpu.VMEM((nz, tok, 2 * depth), b16),
            pltpu.VMEM((ntp - 1, nz, rows, 2 * depth), b16),
            dma((10,)),
            dma((KINDS, 2, half)),
            dma((KINDS, 2, half)),
            dma((KINDS, 3, half)),
            dma((KINDS, 3, half)),
            dma((ntp - 1,)),
            dma((ntp - 1,)),
            dma((ntp - 1,)),
            dma((ntp - 1,)),
            dma((ntp - 1, nz)),
            dma((ntp - 1, nz)),
        ],
        compiler_params=pltpu.CompilerParams(
            collective_id=0, has_side_effects=True, vmem_limit_bytes=60 * 1024 * 1024
        ),
        name="layer",
    )(
        resid_in, queries, keys, values, cum_gate.T, w_out, norm_gain[None, :], w_gate, w_up, w_down.T
    )


def solution(mesh):
    return jax.shard_map(
        functools.partial(on_device, mesh.shape["sp"], mesh.shape["tp"]),
        mesh=mesh,
        in_specs=(
            P(("grp", "sp", "tp"), None),
            P(("grp", "sp"), "tp"),
            P(("grp", "sp"), "tp"),
            P(("grp", "sp"), "tp"),
            P("grp", "tp"),
            P(),
            P(),
            P("sp", "tp"),
            P("sp", "tp"),
            P("tp", "sp"),
        ),
        out_specs=P(("grp", "sp", "tp"), None),
        check_vma=False,
    )
```

```python
import functools

import jax
import jax.numpy as jnp
from jax import lax
from jax.experimental import pallas as pl
from jax.experimental.pallas import tpu as pltpu
from jax.sharding import PartitionSpec as P

HEAD_DIM = 64
NEG = -1e30
K, V, G, U = range(4)
D = tuple(range(4, 8))
KINDS = 8
UP, DOWN, OWN = range(3)
FAR = {kind: kind % 2 for kind in range(KINDS)}
MESH = pl.DeviceIdType.MESH


def kernel(
    nz, ntp,
    resid_in, q_in, k_in, v_in, gate_in, wout_in, gain_in, wg_in, wu_in, wd_in,
    out_ref,
    kbuf, vbuf, wg, wu, wd, qbuf, qm, gate, wout, gain, resid0, resid,
    top, total, acc, att, head_rows, rows, acc_g, acc_u, hidden, terms, psend, precv,
    local_sem, ring_send, ring_recv, pair_send, pair_recv,
    att_send, att_recv, row_send, row_recv, sum_send, sum_recv,
):
    half = nz // 2
    mid = half // 2
    me, t = lax.axis_index("sp"), lax.axis_index("tp")
    z, core = lax.div(me, 2), lax.rem(me, 2)
    partner = me + 1 - 2 * core
    neighbour = (
        2 * lax.rem(z + 1, nz) + core,
        2 * lax.rem(z + nz - 1, nz) + core,
    )
    tok, width = q_in.shape
    heads = width // HEAD_DIM
    own_rows, features = resid_in.shape
    depth, ff = wg_in.shape
    pair = 2 * depth

    def piece(kind, s):
        if kind == K:
            return kbuf.at[s]
        if kind == V:
            return vbuf.at[s]
        if kind == G:
            return wg.at[pl.ds(pl.multiple_of(s * depth, depth), depth)]
        if kind == U:
            return wu.at[pl.ds(pl.multiple_of(s * depth, depth), depth)]
        part = depth // len(D)
        return wd.at[pl.ds(pl.multiple_of(s * depth + part * (kind - D[0]), part), part)]

    def owner(way, dist):
        if way == UP:
            return lax.rem(z + nz - dist, nz)
        return lax.rem(z + dist, nz)

    def ring_copy(kind, way, dist):
        ref = piece(kind, 2 * owner(way, dist - 1) + core)
        return pltpu.make_async_remote_copy(
            ref, ref, ring_send.at[kind, way, dist - 1], ring_recv.at[kind, way, dist - 1],
            device_id={"sp": neighbour[way]}, device_id_type=MESH,
        )

    def ring_wait(kind, way, dist):
        ref = piece(kind, 2 * owner(way, dist) + core)
        pltpu.make_async_remote_copy(
            ref, ref, ring_send.at[kind, way, dist - 1], ring_recv.at[kind, way, dist - 1],
            device_id={"sp": neighbour[way]}, device_id_type=MESH,
        ).wait_recv()

    def pair_copy(kind, way, dist, s):
        ref = piece(kind, s)
        return pltpu.make_async_remote_copy(
            ref, ref, pair_send.at[kind, way, dist - 1], pair_recv.at[kind, way, dist - 1],
            device_id={"sp": partner}, device_id_type=MESH,
        )

    def goes(kind, way, dist, s):
        if kind not in (K, V):
            return True
        if way == UP:
            return s + dist < nz
        return s < (half if FAR[kind] == way else half - 1)

    def used(kind, way, dist):
        return True if kind not in (K, V) else owner(way, dist) < z

    def guard(condition, run):
        if condition is True:
            run()
        else:
            pl.when(condition)(run)

    def own_start(kind):
        for way in (UP, DOWN):
            guard(goes(kind, way, 1, z), lambda way=way: ring_copy(kind, way, 1).start())
        pair_copy(kind, OWN, 1, me).start()

    def arrive(kind, dist):
        for way in (UP, DOWN):
            far = FAR[kind] == way
            s = owner(way, dist)

            def take(way=way, far=far, s=s):
                ring_wait(kind, way, dist)

                @pl.when(dist < (half if far else half - 1))
                def _():
                    guard(goes(kind, way, dist + 1, s), lambda: ring_copy(kind, way, dist + 1).start())

                guard(used(kind, way, dist), lambda: pair_copy(kind, way, dist, 2 * s + core).start())

            comes = goes(kind, way, dist, s)
            if far:
                guard(comes, take)
            else:
                pl.when(dist < half if comes is True else (dist < half) & comes)(take)

    def pair_wait(kind, way, dist):
        if way == OWN:
            pair_copy(kind, OWN, 1, partner).wait_recv()
        else:
            s = 2 * owner(way, dist) + 1 - core
            guard(used(kind, way, dist), lambda: pair_copy(kind, way, dist, s).wait_recv())

    def pair_waits(kinds, dist):
        for kind in kinds:

            @pl.when(dist == 0)
            def _(kind=kind):
                pair_wait(kind, OWN, 1)

            @pl.when(dist == half)
            def _(kind=kind):
                pair_wait(kind, FAR[kind], half)

            @pl.when((dist > 0) & (dist < half))
            def _(kind=kind):
                for way in (UP, DOWN):
                    pair_wait(kind, way, dist)

    def mine(ref):
        return ref.at[pl.ds(pl.multiple_of(me * depth, depth), depth)]

    barrier = pltpu.get_barrier_semaphore()
    peers = [{"sp": neighbour[UP]}, {"sp": neighbour[DOWN]}, {"sp": partner}]
    across = [lax.rem(t + j, ntp) for j in range(1, ntp)]
    peers += [{"tp": other} for other in across]
    for peer in peers:
        pl.semaphore_signal(barrier, inc=1, device_id=peer, device_id_type=MESH)
    loads = [
        (k_in, kbuf.at[me]), (v_in, vbuf.at[me]), (q_in, qbuf), (gate_in, gate),
        (wg_in, mine(wg)), (wu_in, mine(wu)), (wd_in, mine(wd)),
        (resid_in, resid0), (wout_in, wout), (gain_in, gain),
    ]
    load = [pltpu.make_async_copy(a, b, local_sem.at[i]) for i, (a, b) in enumerate(loads)]
    for copy in load:
        copy.start()
    pl.semaphore_wait(barrier, len(peers))

    load[0].wait()
    own_start(K)
    load[1].wait()
    own_start(V)
    load[4].wait()
    own_start(G)
    load[5].wait()
    own_start(U)
    load[2].wait()
    load[3].wait()

    turned = (qbuf[...].astype(jnp.float32).T * HEAD_DIM ** (-0.5)).astype(jnp.bfloat16)
    nothing = jnp.zeros((HEAD_DIM, tok), jnp.bfloat16)
    for h in range(heads):
        mine_h = turned[h * HEAD_DIM : (h + 1) * HEAD_DIM]
        qm[h] = jnp.concatenate([mine_h, nothing] if h % 2 == 0 else [nothing, mine_h], axis=0)
    top[...] = jnp.full_like(top, NEG)
    total[...] = jnp.zeros_like(total)
    acc[...] = jnp.zeros_like(acc)

    def attend(s, diagonal):
        key_rows = kbuf[s]
        turned_values = vbuf[s].T
        bias = gate[:, pl.ds(pl.multiple_of(s * tok, tok), tok)]
        bias = jnp.concatenate([bias] * (8 // heads), axis=0).T
        for h in range(heads):
            lanes = slice(h // 2 * 128, h // 2 * 128 + 128)
            scores = jnp.dot(key_rows[:, lanes], qm[h], preferred_element_type=jnp.float32)
            scores = scores - bias[:, h : h + 1]
            if diagonal:
                at = lax.broadcasted_iota(jnp.int32, scores.shape, 0)
                scores = jnp.where(at <= lax.broadcasted_iota(jnp.int32, scores.shape, 1), scores, NEG)
            before = top[h : h + 1, :]
            now = jnp.maximum(before, jnp.max(scores, axis=0, keepdims=True))
            weights = jnp.exp(scores - now)
            rescale = jnp.exp(before - now)
            top[h : h + 1, :] = now
            total[h : h + 1, :] = total[h : h + 1, :] * rescale + jnp.sum(weights, axis=0, keepdims=True)
            part = slice(h * HEAD_DIM, (h + 1) * HEAD_DIM)
            product = jnp.dot(
                turned_values[part], weights.astype(jnp.bfloat16), preferred_element_type=jnp.float32
            )
            acc[part] = acc[part] * rescale + product

    attend(me, True)

    def attention_step(dist, carry):
        @pl.when(dist <= half)
        def _():
            arrive(K, dist)
            arrive(V, dist)

        @pl.when((dist > 1) & (dist <= half))
        def _():
            pl.when(lax.rem(dist, 2) == 0)(lambda: arrive(G, lax.div(dist, 2)))
            pl.when(lax.rem(dist, 2) == 1)(lambda: arrive(U, lax.div(dist, 2)))

        @pl.when(dist == half)
        def _():
            load[6].wait()
            for kind in D:
                own_start(kind)

        last = dist - 1
        pair_waits((K, V), last)

        def job(j, carry):
            way, par = lax.div(j, 2), lax.rem(j, 2)
            zb = lax.rem(z + nz + last * (2 * way - 1), nz)
            s = 2 * zb + core + par * (1 - 2 * core)

            @pl.when(s < me)
            def _():
                attend(s, False)

            return carry

        jobs = 4 - 2 * (lax.div(last, half) + lax.div(half - last, half))
        return lax.fori_loop(0, jobs, job, carry)

    lax.fori_loop(1, half + 2, attention_step, 0)

    sums = jnp.concatenate(
        [
            acc[h * HEAD_DIM : (h + 1) * HEAD_DIM] / total[h : h + 1, :]
            for h in range(heads)
        ],
        axis=0,
    )
    att[...] = sums.T.astype(jnp.bfloat16)

    def rows_of(ref, which):
        return ref.at[pl.ds(pl.multiple_of(which * own_rows, own_rows), own_rows)]

    def att_copy(j):
        return pltpu.make_async_remote_copy(
            rows_of(att, across[j]), head_rows.at[t], att_send.at[j], att_recv.at[j],
            device_id={"tp": across[j]}, device_id_type=MESH,
        )

    def att_wait(j):
        source = lax.rem(t + ntp - 1 - j, ntp)
        pltpu.make_async_remote_copy(
            rows_of(att, across[j]), head_rows.at[source], att_send.at[j], att_recv.at[j],
            device_id={"tp": across[j]}, device_id_type=MESH,
        ).wait_recv()

    for j in range(ntp - 1):
        att_copy(j).start()
    arrive(U, mid)
    head_rows[t] = att[pl.ds(pl.multiple_of(t * own_rows, own_rows), own_rows), :]
    load[7].wait()
    load[8].wait()
    load[9].wait()
    acc_g[...] = jnp.zeros_like(acc_g)
    acc_u[...] = jnp.zeros_like(acc_u)
    for j in range(ntp - 1):
        att_wait(j)
    tile = 256
    squares = jnp.zeros((own_rows, tile), jnp.float32)
    for i in range(features // tile):
        part = slice(i * tile, (i + 1) * tile)
        mixed = jnp.zeros((own_rows, tile), jnp.float32)
        for j in range(ntp):
            mixed += jnp.dot(
                head_rows[j], wout[j * width : (j + 1) * width, part],
                preferred_element_type=jnp.float32,
            )
        mixed = resid0[:, part].astype(jnp.float32) + mixed
        resid[:, part] = mixed
        squares += mixed * mixed
    scale = lax.rsqrt(jnp.sum(squares, axis=1, keepdims=True) / features + 1e-06)
    at_rows = pl.ds(pl.multiple_of(t * own_rows, own_rows), own_rows)
    rows[at_rows, :] = (resid[...] * scale * gain[...]).astype(jnp.bfloat16)

    def row_copy(j, which):
        return pltpu.make_async_remote_copy(
            rows_of(rows, which), rows_of(rows, which), row_send.at[j], row_recv.at[j],
            device_id={"tp": across[j]}, device_id_type=MESH,
        )

    def forward_down(dist):
        for kind in D:
            arrive(kind, dist)

    arrive(G, mid + 1)
    for j in range(ntp - 1):
        row_copy(j, t).start()

    def place(index):
        dist = lax.div(index + 1, 2)
        return dist, lax.rem(z + nz + dist * (1 - 2 * lax.rem(index, 2)), nz)

    def pair_ready(kinds, index, dist):
        for kind in kinds:

            @pl.when(dist == 0)
            def _(kind=kind):
                pair_wait(kind, OWN, 1)

            @pl.when(dist == half)
            def _(kind=kind):
                pair_wait(kind, FAR[kind], half)

            for way in (UP, DOWN):

                @pl.when((dist > 0) & (dist < half) & (lax.rem(index, 2) == 1 - way))
                def _(kind=kind, way=way):
                    pair_wait(kind, way, dist)

    first, turns = mid + 2, 6

    def up_done(dist):
        return jnp.clip(jnp.minimum(turns * (dist - first + 1), 2 * dist - 1), 0, nz)

    def up_step(dist, carry):
        def turn(j, carry):
            @pl.when((j == 0) & (dist <= half))
            def _():
                arrive(U, dist)

            @pl.when((j == 2) & (dist < half))
            def _():
                arrive(G, dist + 1)

            @pl.when((j == 4) & (dist > mid + 1) & (dist <= half))
            def _():
                forward_down(dist - mid - 1)

            @pl.when((j == 4) & (dist == half - 1))
            def _():
                for i in range(ntp - 1):
                    att_copy(i).wait_send()

            @pl.when((j == 0) & (dist == first))
            def _():
                for i in range(ntp - 1):
                    row_copy(i, lax.rem(t + ntp - 1 - i, ntp)).wait_recv()

            index = up_done(dist - 1) + j

            @pl.when(index < up_done(dist))
            def _():
                away, zb = place(index)
                pair_ready((G, U), index, away)
                block = pl.ds(pl.multiple_of(zb * pair, pair), pair)
                left = rows[:, block]
                acc_g[...] += jnp.dot(left, wg[block, :], preferred_element_type=jnp.float32)
                acc_u[...] += jnp.dot(left, wu[block, :], preferred_element_type=jnp.float32)

            return carry

        return lax.fori_loop(0, turns, turn, carry)

    lax.fori_loop(mid + 1, half + 2, up_step, 0)

    def activate(i, carry):
        part = pl.ds(pl.multiple_of(i * 16, 16), 16)
        g = acc_g[part, :]
        hidden[part, :] = (g / (1.0 + jnp.exp(-g)) * acc_u[part, :]).astype(jnp.bfloat16)
        return carry

    lax.fori_loop(0, tok // 16, activate, 0)

    def sum_copy(j, zb):
        return pltpu.make_async_remote_copy(
            psend.at[zb, pl.ds(pl.multiple_of(across[j] * own_rows, own_rows), own_rows)],
            precv.at[j, zb], sum_send.at[j, zb], sum_recv.at[j, zb],
            device_id={"tp": across[j]}, device_id_type=MESH,
        )

    start = half - mid

    def down_done(dist):
        return jnp.clip(jnp.minimum(len(D) * (dist - start + 1), 2 * dist - 1), 0, nz)

    def sent(kinds, begin, end):
        for kind in kinds:
            for way in (UP, DOWN):

                def left(dist, carry, kind=kind, way=way):
                    guard(
                        goes(kind, way, dist, owner(way, dist - 1)),
                        lambda: ring_copy(kind, way, dist).wait_send(),
                    )
                    guard(
                        used(kind, way, dist),
                        lambda: pair_copy(kind, way, dist, 2 * owner(way, dist) + core).wait_send(),
                    )
                    return carry

                reach = half if FAR[kind] == way else half - 1
                lax.fori_loop(begin, min(end, reach + 1), left, 0)

    def down_step(dist, carry):
        def turn(j, carry):
            for i, kind in enumerate(D):

                @pl.when((j == i) & (dist <= half))
                def _(kind=kind):
                    arrive(kind, dist)

            index = down_done(dist - 1) + j

            @pl.when(index < down_done(dist))
            def _():
                away, zb = place(index)
                pair_ready(D, index, away)
                block = pl.ds(pl.multiple_of(zb * pair, pair), pair)
                terms[...] = lax.dot_general(
                    hidden[...], wd[block, :], (((1,), (1,)), ((), ())),
                    preferred_element_type=jnp.float32,
                )
                psend[zb] = terms[...].astype(jnp.bfloat16)
                resid[:, block] += terms[at_rows, :]
                for i in sorted(range(ntp - 1), key=lambda i: -min(i + 1, ntp - 1 - i)):
                    sum_copy(i, zb).start()

            return carry

        lax.fori_loop(0, len(D), turn, 0)

        @pl.when(dist == start)
        def _():
            for j in range(ntp - 1):
                row_copy(j, t).wait_send()
            for kind in range(KINDS):
                pair_copy(kind, OWN, 1, me).wait_send()
            sent((K, V), 1, half + 1)

        pl.when(dist == start + 1)(lambda: sent((G,), 1, half + 1))
        pl.when(dist == start + 2)(lambda: sent((U,), 1, half + 1))
        pl.when(dist == half - 1)(lambda: sent(D, 1, half - 1))
        pl.when(dist == half)(lambda: sent(D, half - 1, half))

        def finish(index, carry):
            _, zb = place(index)
            block = pl.ds(pl.multiple_of(zb * pair, pair), pair)
            value = resid[:, block]
            for j in range(ntp - 1):
                sum_copy(j, zb).wait_recv()
                sum_copy(j, zb).wait_send()
                value += precv[j, zb].astype(jnp.float32)
            out_ref[:, block] = value.astype(jnp.bfloat16)
            return carry

        return lax.fori_loop(down_done(dist - 2), down_done(dist - 1), finish, carry)

    lax.fori_loop(start, half + 3, down_step, 0)

    for kind in D:
        sent((kind,), half, half + 1)


def on_device(nsp, ntp, resid_in, queries, keys, values, cum_gate, w_out, norm_gain, w_gate, w_up, w_down):
    nz = nsp // 2
    half = nz // 2
    tok, width = queries.shape
    rows, features = resid_in.shape
    depth, ff = w_gate.shape
    heads = width // HEAD_DIM
    b16, f32 = jnp.bfloat16, jnp.float32
    dma = pltpu.SemaphoreType.DMA
    return pl.pallas_call(
        functools.partial(kernel, nz, ntp),
        out_shape=pltpu.VMEM((rows, features), b16),
        in_specs=[pl.BlockSpec(memory_space=pl.ANY)] * 10,
        out_specs=pl.BlockSpec(memory_space=pltpu.VMEM),
        scratch_shapes=[
            pltpu.VMEM((nsp, tok, width), b16),
            pltpu.VMEM((nsp, tok, width), b16),
            pltpu.VMEM((nsp * depth, ff), b16),
            pltpu.VMEM((nsp * depth, ff), b16),
            pltpu.VMEM((nsp * depth, ff), b16),
            pltpu.VMEM((tok, width), b16),
            pltpu.VMEM((heads, 128, tok), b16),
            pltpu.VMEM((heads, nsp * tok), f32),
            pltpu.VMEM(w_out.shape, b16),
            pltpu.VMEM((1, features), f32),
            pltpu.VMEM((rows, features), b16),
            pltpu.VMEM((rows, features), f32),
            pltpu.VMEM((heads, tok), f32),
            pltpu.VMEM((heads, tok), f32),
            pltpu.VMEM((width, tok), f32),
            pltpu.VMEM((tok, width), b16),
            pltpu.VMEM((ntp, rows, width), b16),
            pltpu.VMEM((tok, features), b16),
            pltpu.VMEM((tok, ff), f32),
            pltpu.VMEM((tok, ff), f32),
            pltpu.VMEM((tok, ff), b16),
            pltpu.VMEM((tok, 2 * depth), f32),
            pltpu.VMEM((nz, tok, 2 * depth), b16),
            pltpu.VMEM((ntp - 1, nz, rows, 2 * depth), b16),
            dma((10,)),
            dma((KINDS, 2, half)),
            dma((KINDS, 2, half)),
            dma((KINDS, 3, half)),
            dma((KINDS, 3, half)),
            dma((ntp - 1,)),
            dma((ntp - 1,)),
            dma((ntp - 1,)),
            dma((ntp - 1,)),
            dma((ntp - 1, nz)),
            dma((ntp - 1, nz)),
        ],
        compiler_params=pltpu.CompilerParams(
            collective_id=0, has_side_effects=True, vmem_limit_bytes=60 * 1024 * 1024
        ),
        name="layer",
    )(
        resid_in, queries, keys, values, cum_gate.T, w_out, norm_gain[None, :], w_gate, w_up, w_down.T
    )


def solution(mesh):
    return jax.shard_map(
        functools.partial(on_device, mesh.shape["sp"], mesh.shape["tp"]),
        mesh=mesh,
        in_specs=(
            P(("grp", "sp", "tp"), None),
            P(("grp", "sp"), "tp"),
            P(("grp", "sp"), "tp"),
            P(("grp", "sp"), "tp"),
            P("grp", "tp"),
            P(),
            P(),
            P("sp", "tp"),
            P("sp", "tp"),
            P("tp", "sp"),
        ),
        out_specs=P(("grp", "sp", "tp"), None),
        check_vma=False,
    )
```

```python
import functools

import jax
import jax.numpy as jnp
from jax import lax
from jax.experimental import pallas as pl
from jax.experimental.pallas import tpu as pltpu
from jax.sharding import PartitionSpec as P

HEAD_DIM = 64
NEG = -1e30
K, V, G, U = range(4)
D = tuple(range(4, 8))
KINDS = 8
UP, DOWN, OWN = range(3)
FAR = {kind: kind % 2 for kind in range(KINDS)}
MESH = pl.DeviceIdType.MESH


def kernel(
    nz, ntp,
    resid_in, q_in, k_in, v_in, gate_in, wout_in, gain_in, wg_in, wu_in, wd_in,
    out_ref,
    kbuf, vbuf, wg, wu, wd, qbuf, qm, gate, wout, gain, resid0, resid,
    top, total, acc, att, head_rows, rows, acc_g, acc_u, hidden, terms, psend, precv,
    local_sem, ring_send, ring_recv, pair_send, pair_recv,
    att_send, att_recv, row_send, row_recv, sum_send, sum_recv,
):
    half = nz // 2
    mid = half // 2
    me, t = lax.axis_index("sp"), lax.axis_index("tp")
    z, core = lax.div(me, 2), lax.rem(me, 2)
    partner = me + 1 - 2 * core
    neighbour = (
        2 * lax.rem(z + 1, nz) + core,
        2 * lax.rem(z + nz - 1, nz) + core,
    )
    tok, width = q_in.shape
    heads = width // HEAD_DIM
    own_rows, features = resid_in.shape
    depth, ff = wg_in.shape
    pair = 2 * depth

    def piece(kind, s):
        if kind == K:
            return kbuf.at[s]
        if kind == V:
            return vbuf.at[s]
        if kind == G:
            return wg.at[pl.ds(pl.multiple_of(s * depth, depth), depth)]
        if kind == U:
            return wu.at[pl.ds(pl.multiple_of(s * depth, depth), depth)]
        part = depth // len(D)
        return wd.at[pl.ds(pl.multiple_of(s * depth + part * (kind - D[0]), part), part)]

    def owner(way, dist):
        if way == UP:
            return lax.rem(z + nz - dist, nz)
        return lax.rem(z + dist, nz)

    def ring_copy(kind, way, dist):
        ref = piece(kind, 2 * owner(way, dist - 1) + core)
        return pltpu.make_async_remote_copy(
            ref, ref, ring_send.at[kind, way, dist - 1], ring_recv.at[kind, way, dist - 1],
            device_id={"sp": neighbour[way]}, device_id_type=MESH,
        )

    def ring_wait(kind, way, dist):
        ref = piece(kind, 2 * owner(way, dist) + core)
        pltpu.make_async_remote_copy(
            ref, ref, ring_send.at[kind, way, dist - 1], ring_recv.at[kind, way, dist - 1],
            device_id={"sp": neighbour[way]}, device_id_type=MESH,
        ).wait_recv()

    def pair_copy(kind, way, dist, s):
        ref = piece(kind, s)
        return pltpu.make_async_remote_copy(
            ref, ref, pair_send.at[kind, way, dist - 1], pair_recv.at[kind, way, dist - 1],
            device_id={"sp": partner}, device_id_type=MESH,
        )

    def goes(kind, way, dist, s):
        if kind not in (K, V):
            return True
        if way == UP:
            return s + dist < nz
        return s < (half if FAR[kind] == way else half - 1)

    def used(kind, way, dist):
        return True if kind not in (K, V) else owner(way, dist) < z

    def guard(condition, run):
        if condition is True:
            run()
        else:
            pl.when(condition)(run)

    def own_start(kind):
        for way in (UP, DOWN):
            guard(goes(kind, way, 1, z), lambda way=way: ring_copy(kind, way, 1).start())
        pair_copy(kind, OWN, 1, me).start()

    def arrive(kind, dist):
        for way in (UP, DOWN):
            far = FAR[kind] == way
            s = owner(way, dist)

            def take(way=way, far=far, s=s):
                ring_wait(kind, way, dist)

                @pl.when(dist < (half if far else half - 1))
                def _():
                    guard(goes(kind, way, dist + 1, s), lambda: ring_copy(kind, way, dist + 1).start())

            comes = goes(kind, way, dist, s)
            if far:
                guard(comes, take)
            else:
                pl.when(dist < half if comes is True else (dist < half) & comes)(take)

        for way in (UP, DOWN):

            def hand(way=way):
                pair_copy(kind, way, dist, 2 * owner(way, dist) + core).start()

            wanted = used(kind, way, dist)
            if FAR[kind] == way:
                guard(wanted, hand)
            else:
                pl.when(dist < half if wanted is True else (dist < half) & wanted)(hand)

    def pair_wait(kind, way, dist):
        if way == OWN:
            pair_copy(kind, OWN, 1, partner).wait_recv()
        else:
            s = 2 * owner(way, dist) + 1 - core
            guard(used(kind, way, dist), lambda: pair_copy(kind, way, dist, s).wait_recv())

    def pair_waits(kinds, dist):
        for kind in kinds:

            @pl.when(dist == 0)
            def _(kind=kind):
                pair_wait(kind, OWN, 1)

            @pl.when(dist == half)
            def _(kind=kind):
                pair_wait(kind, FAR[kind], half)

            @pl.when((dist > 0) & (dist < half))
            def _(kind=kind):
                for way in (UP, DOWN):
                    pair_wait(kind, way, dist)

    def mine(ref):
        return ref.at[pl.ds(pl.multiple_of(me * depth, depth), depth)]

    barrier = pltpu.get_barrier_semaphore()
    peers = [{"sp": neighbour[UP]}, {"sp": neighbour[DOWN]}, {"sp": partner}]
    across = [lax.rem(t + j, ntp) for j in range(1, ntp)]
    peers += [{"tp": other} for other in across]
    for peer in peers:
        pl.semaphore_signal(barrier, inc=1, device_id=peer, device_id_type=MESH)
    loads = [
        (k_in, kbuf.at[me]), (v_in, vbuf.at[me]), (q_in, qbuf), (gate_in, gate),
        (wg_in, mine(wg)), (wu_in, mine(wu)), (wd_in, mine(wd)),
        (resid_in, resid0), (wout_in, wout), (gain_in, gain),
    ]
    load = [pltpu.make_async_copy(a, b, local_sem.at[i]) for i, (a, b) in enumerate(loads)]
    for copy in load:
        copy.start()
    pl.semaphore_wait(barrier, len(peers))

    load[0].wait()
    own_start(K)
    load[1].wait()
    own_start(V)
    load[4].wait()
    own_start(G)
    load[5].wait()
    own_start(U)
    load[2].wait()
    load[3].wait()

    turned = (qbuf[...].astype(jnp.float32).T * HEAD_DIM ** (-0.5)).astype(jnp.bfloat16)
    nothing = jnp.zeros((HEAD_DIM, tok), jnp.bfloat16)
    for h in range(heads):
        mine_h = turned[h * HEAD_DIM : (h + 1) * HEAD_DIM]
        qm[h] = jnp.concatenate([mine_h, nothing] if h % 2 == 0 else [nothing, mine_h], axis=0)
    top[...] = jnp.full_like(top, NEG)
    total[...] = jnp.zeros_like(total)
    acc[...] = jnp.zeros_like(acc)

    def attend(s, diagonal):
        key_rows = kbuf[s]
        turned_values = vbuf[s].T
        bias = gate[:, pl.ds(pl.multiple_of(s * tok, tok), tok)]
        bias = jnp.concatenate([bias] * (8 // heads), axis=0).T
        for h in range(heads):
            lanes = slice(h // 2 * 128, h // 2 * 128 + 128)
            scores = jnp.dot(key_rows[:, lanes], qm[h], preferred_element_type=jnp.float32)
            scores = scores - bias[:, h : h + 1]
            if diagonal:
                at = lax.broadcasted_iota(jnp.int32, scores.shape, 0)
                scores = jnp.where(at <= lax.broadcasted_iota(jnp.int32, scores.shape, 1), scores, NEG)
            before = top[h : h + 1, :]
            now = jnp.maximum(before, jnp.max(scores, axis=0, keepdims=True))
            weights = jnp.exp(scores - now)
            rescale = jnp.exp(before - now)
            top[h : h + 1, :] = now
            total[h : h + 1, :] = total[h : h + 1, :] * rescale + jnp.sum(weights, axis=0, keepdims=True)
            part = slice(h * HEAD_DIM, (h + 1) * HEAD_DIM)
            product = jnp.dot(
                turned_values[part], weights.astype(jnp.bfloat16), preferred_element_type=jnp.float32
            )
            acc[part] = acc[part] * rescale + product

    attend(me, True)

    def attention_step(dist, carry):
        @pl.when(dist <= half)
        def _():
            arrive(K, dist)
            arrive(V, dist)

        @pl.when((dist > 1) & (dist <= half))
        def _():
            pl.when(lax.rem(dist, 2) == 0)(lambda: arrive(G, lax.div(dist, 2)))
            pl.when(lax.rem(dist, 2) == 1)(lambda: arrive(U, lax.div(dist, 2)))

        @pl.when(dist == half)
        def _():
            load[6].wait()
            for kind in D:
                own_start(kind)

        last = dist - 1
        pair_waits((K, V), last)

        def job(j, carry):
            way, par = lax.div(j, 2), lax.rem(j, 2)
            zb = lax.rem(z + nz + last * (2 * way - 1), nz)
            s = 2 * zb + core + par * (1 - 2 * core)

            @pl.when(s < me)
            def _():
                attend(s, False)

            return carry

        jobs = 4 - 2 * (lax.div(last, half) + lax.div(half - last, half))
        return lax.fori_loop(0, jobs, job, carry)

    lax.fori_loop(1, half + 2, attention_step, 0)

    sums = jnp.concatenate(
        [
            acc[h * HEAD_DIM : (h + 1) * HEAD_DIM] / total[h : h + 1, :]
            for h in range(heads)
        ],
        axis=0,
    )
    att[...] = sums.T.astype(jnp.bfloat16)

    def rows_of(ref, which):
        return ref.at[pl.ds(pl.multiple_of(which * own_rows, own_rows), own_rows)]

    def att_copy(j):
        return pltpu.make_async_remote_copy(
            rows_of(att, across[j]), head_rows.at[t], att_send.at[j], att_recv.at[j],
            device_id={"tp": across[j]}, device_id_type=MESH,
        )

    def att_wait(j):
        source = lax.rem(t + ntp - 1 - j, ntp)
        pltpu.make_async_remote_copy(
            rows_of(att, across[j]), head_rows.at[source], att_send.at[j], att_recv.at[j],
            device_id={"tp": across[j]}, device_id_type=MESH,
        ).wait_recv()

    for j in range(ntp - 1):
        att_copy(j).start()
    arrive(U, mid)
    head_rows[t] = att[pl.ds(pl.multiple_of(t * own_rows, own_rows), own_rows), :]
    load[7].wait()
    load[8].wait()
    load[9].wait()
    acc_g[...] = jnp.zeros_like(acc_g)
    acc_u[...] = jnp.zeros_like(acc_u)
    for j in range(ntp - 1):
        att_wait(j)
    tile = 256
    squares = jnp.zeros((own_rows, tile), jnp.float32)
    for i in range(features // tile):
        part = slice(i * tile, (i + 1) * tile)
        mixed = jnp.zeros((own_rows, tile), jnp.float32)
        for j in range(ntp):
            mixed += jnp.dot(
                head_rows[j], wout[j * width : (j + 1) * width, part],
                preferred_element_type=jnp.float32,
            )
        mixed = resid0[:, part].astype(jnp.float32) + mixed
        resid[:, part] = mixed
        squares += mixed * mixed
    scale = lax.rsqrt(jnp.sum(squares, axis=1, keepdims=True) / features + 1e-06)
    at_rows = pl.ds(pl.multiple_of(t * own_rows, own_rows), own_rows)
    rows[at_rows, :] = (resid[...] * scale * gain[...]).astype(jnp.bfloat16)

    def row_copy(j, which):
        return pltpu.make_async_remote_copy(
            rows_of(rows, which), rows_of(rows, which), row_send.at[j], row_recv.at[j],
            device_id={"tp": across[j]}, device_id_type=MESH,
        )

    def forward_down(dist):
        for kind in D:
            arrive(kind, dist)

    arrive(G, mid + 1)
    for j in range(ntp - 1):
        row_copy(j, t).start()

    def place(index):
        dist = lax.div(index + 1, 2)
        return dist, lax.rem(z + nz + dist * (1 - 2 * lax.rem(index, 2)), nz)

    def pair_ready(kinds, index, dist):
        for kind in kinds:

            @pl.when(dist == 0)
            def _(kind=kind):
                pair_wait(kind, OWN, 1)

            @pl.when(dist == half)
            def _(kind=kind):
                pair_wait(kind, FAR[kind], half)

            for way in (UP, DOWN):

                @pl.when((dist > 0) & (dist < half) & (lax.rem(index, 2) == 1 - way))
                def _(kind=kind, way=way):
                    pair_wait(kind, way, dist)

    first, turns = mid + 2, 6

    def up_done(dist):
        return jnp.clip(jnp.minimum(turns * (dist - first + 1), 2 * dist - 1), 0, nz)

    def up_step(dist, carry):
        def turn(j, carry):
            @pl.when((j == 0) & (dist <= half))
            def _():
                arrive(U, dist)

            @pl.when((j == 2) & (dist < half))
            def _():
                arrive(G, dist + 1)

            @pl.when((j == 4) & (dist > mid + 1) & (dist <= half))
            def _():
                forward_down(dist - mid - 1)

            @pl.when((j == 4) & (dist == half - 1))
            def _():
                for i in range(ntp - 1):
                    att_copy(i).wait_send()

            @pl.when((j == 0) & (dist == first))
            def _():
                for i in range(ntp - 1):
                    row_copy(i, lax.rem(t + ntp - 1 - i, ntp)).wait_recv()

            index = up_done(dist - 1) + j

            @pl.when(index < up_done(dist))
            def _():
                away, zb = place(index)
                pair_ready((G, U), index, away)
                block = pl.ds(pl.multiple_of(zb * pair, pair), pair)
                left = rows[:, block]
                acc_g[...] += jnp.dot(left, wg[block, :], preferred_element_type=jnp.float32)
                acc_u[...] += jnp.dot(left, wu[block, :], preferred_element_type=jnp.float32)

            return carry

        return lax.fori_loop(0, turns, turn, carry)

    lax.fori_loop(mid + 1, half + 2, up_step, 0)

    def activate(i, carry):
        part = pl.ds(pl.multiple_of(i * 16, 16), 16)
        g = acc_g[part, :]
        hidden[part, :] = (g / (1.0 + jnp.exp(-g)) * acc_u[part, :]).astype(jnp.bfloat16)
        return carry

    lax.fori_loop(0, tok // 16, activate, 0)

    def sum_copy(j, zb):
        return pltpu.make_async_remote_copy(
            psend.at[zb, pl.ds(pl.multiple_of(across[j] * own_rows, own_rows), own_rows)],
            precv.at[j, zb], sum_send.at[j, zb], sum_recv.at[j, zb],
            device_id={"tp": across[j]}, device_id_type=MESH,
        )

    start = half - mid

    def down_done(dist):
        return jnp.clip(jnp.minimum(len(D) * (dist - start + 1), 2 * dist - 1), 0, nz)

    def sent(kinds, begin, end):
        for kind in kinds:
            for way in (UP, DOWN):

                def left(dist, carry, kind=kind, way=way):
                    guard(
                        goes(kind, way, dist, owner(way, dist - 1)),
                        lambda: ring_copy(kind, way, dist).wait_send(),
                    )
                    guard(
                        used(kind, way, dist),
                        lambda: pair_copy(kind, way, dist, 2 * owner(way, dist) + core).wait_send(),
                    )
                    return carry

                reach = half if FAR[kind] == way else half - 1
                lax.fori_loop(begin, min(end, reach + 1), left, 0)

    def down_step(dist, carry):
        def turn(j, carry):
            for i, kind in enumerate(D):

                @pl.when((j == i) & (dist <= half))
                def _(kind=kind):
                    arrive(kind, dist)

            index = down_done(dist - 1) + j

            @pl.when(index < down_done(dist))
            def _():
                away, zb = place(index)
                pair_ready(D, index, away)
                block = pl.ds(pl.multiple_of(zb * pair, pair), pair)
                terms[...] = lax.dot_general(
                    hidden[...], wd[block, :], (((1,), (1,)), ((), ())),
                    preferred_element_type=jnp.float32,
                )
                psend[zb] = terms[...].astype(jnp.bfloat16)
                resid[:, block] += terms[at_rows, :]
                for i in sorted(range(ntp - 1), key=lambda i: -min(i + 1, ntp - 1 - i)):
                    sum_copy(i, zb).start()

            return carry

        lax.fori_loop(0, len(D), turn, 0)

        @pl.when(dist == start)
        def _():
            for j in range(ntp - 1):
                row_copy(j, t).wait_send()
            for kind in range(KINDS):
                pair_copy(kind, OWN, 1, me).wait_send()
            sent((K, V), 1, half + 1)

        pl.when(dist == start + 1)(lambda: sent((G,), 1, half + 1))
        pl.when(dist == start + 2)(lambda: sent((U,), 1, half + 1))
        pl.when(dist == half - 1)(lambda: sent(D, 1, half - 1))
        pl.when(dist == half)(lambda: sent(D, half - 1, half))

        def finish(index, carry):
            _, zb = place(index)
            block = pl.ds(pl.multiple_of(zb * pair, pair), pair)
            value = resid[:, block]
            for j in range(ntp - 1):
                sum_copy(j, zb).wait_recv()
                sum_copy(j, zb).wait_send()
                value += precv[j, zb].astype(jnp.float32)
            out_ref[:, block] = value.astype(jnp.bfloat16)
            return carry

        return lax.fori_loop(down_done(dist - 2), down_done(dist - 1), finish, carry)

    lax.fori_loop(start, half + 3, down_step, 0)

    for kind in D:
        sent((kind,), half, half + 1)


def on_device(nsp, ntp, resid_in, queries, keys, values, cum_gate, w_out, norm_gain, w_gate, w_up, w_down):
    nz = nsp // 2
    half = nz // 2
    tok, width = queries.shape
    rows, features = resid_in.shape
    depth, ff = w_gate.shape
    heads = width // HEAD_DIM
    b16, f32 = jnp.bfloat16, jnp.float32
    dma = pltpu.SemaphoreType.DMA
    return pl.pallas_call(
        functools.partial(kernel, nz, ntp),
        out_shape=pltpu.VMEM((rows, features), b16),
        in_specs=[pl.BlockSpec(memory_space=pl.ANY)] * 10,
        out_specs=pl.BlockSpec(memory_space=pltpu.VMEM),
        scratch_shapes=[
            pltpu.VMEM((nsp, tok, width), b16),
            pltpu.VMEM((nsp, tok, width), b16),
            pltpu.VMEM((nsp * depth, ff), b16),
            pltpu.VMEM((nsp * depth, ff), b16),
            pltpu.VMEM((nsp * depth, ff), b16),
            pltpu.VMEM((tok, width), b16),
            pltpu.VMEM((heads, 128, tok), b16),
            pltpu.VMEM((heads, nsp * tok), f32),
            pltpu.VMEM(w_out.shape, b16),
            pltpu.VMEM((1, features), f32),
            pltpu.VMEM((rows, features), b16),
            pltpu.VMEM((rows, features), f32),
            pltpu.VMEM((heads, tok), f32),
            pltpu.VMEM((heads, tok), f32),
            pltpu.VMEM((width, tok), f32),
            pltpu.VMEM((tok, width), b16),
            pltpu.VMEM((ntp, rows, width), b16),
            pltpu.VMEM((tok, features), b16),
            pltpu.VMEM((tok, ff), f32),
            pltpu.VMEM((tok, ff), f32),
            pltpu.VMEM((tok, ff), b16),
            pltpu.VMEM((tok, 2 * depth), f32),
            pltpu.VMEM((nz, tok, 2 * depth), b16),
            pltpu.VMEM((ntp - 1, nz, rows, 2 * depth), b16),
            dma((10,)),
            dma((KINDS, 2, half)),
            dma((KINDS, 2, half)),
            dma((KINDS, 3, half)),
            dma((KINDS, 3, half)),
            dma((ntp - 1,)),
            dma((ntp - 1,)),
            dma((ntp - 1,)),
            dma((ntp - 1,)),
            dma((ntp - 1, nz)),
            dma((ntp - 1, nz)),
        ],
        compiler_params=pltpu.CompilerParams(
            collective_id=0, has_side_effects=True, vmem_limit_bytes=60 * 1024 * 1024
        ),
        name="layer",
    )(
        resid_in, queries, keys, values, cum_gate.T, w_out, norm_gain[None, :], w_gate, w_up, w_down.T
    )


def solution(mesh):
    return jax.shard_map(
        functools.partial(on_device, mesh.shape["sp"], mesh.shape["tp"]),
        mesh=mesh,
        in_specs=(
            P(("grp", "sp", "tp"), None),
            P(("grp", "sp"), "tp"),
            P(("grp", "sp"), "tp"),
            P(("grp", "sp"), "tp"),
            P("grp", "tp"),
            P(),
            P(),
            P("sp", "tp"),
            P("sp", "tp"),
            P("tp", "sp"),
        ),
        out_specs=P(("grp", "sp", "tp"), None),
        check_vma=False,
    )
```
